32 devices in a mesh: ep: 16 (over z, y, x), tp: 2 (over core).
Axes of the slice: x: 2, y: 2, z: 4, core: 2. Of those that a mesh axis runs over, the one named last changes fastest.
Arguments:
- hidden: bfloat16 [256, 2048], P('ep'), may hold values from -6 to 6
- attn_gain: bfloat16 [2048], replicated, may hold values from 0.099609375 to 1.8984375
- query_weight: bfloat16 [2048, 2048], P(None, 'tp'), may hold values from -0.125 to 0.125
- key_weight: bfloat16 [2048, 128], P(None, 'tp'), may hold values from -0.125 to 0.125
- value_weight: bfloat16 [2048, 128], P(None, 'tp'), may hold values from -0.125 to 0.125
- forget_weight: bfloat16 [2048, 32], P(None, 'tp'), may hold values from -0.125 to 0.125
- forget_bias: float32 [32], P('tp'), may hold values from -1 to 4
- cache_keys: bfloat16 [256, 2, 64, 1024], P('ep', 'tp'), may hold values from -64 to 64
- cache_values: bfloat16 [256, 2, 64, 1024], P('ep', 'tp'), may hold values from -6 to 6
- cache_logsum: float32 [256, 32, 1024], P('ep', 'tp'), may hold values from -144 to 0, as said below
- lengths: int32 [256], P('ep'), may hold values from 2 to 1023, as said below
- out_weight: bfloat16 [2048, 2048], P('ep'), may hold values from -0.125 to 0.125
- ffn_gain: bfloat16 [2048], replicated, may hold values from 0.099609375 to 1.8984375
- expert_ids: int32 [256, 6], P('ep'), may hold values from 0 to 15, all different within a row; in each aligned block of 16 rows (0 to 15, 16 to 31, ...) at most 12 rows name the same one
- expert_scores: float32 [256, 6], P('ep'), may hold values from 0.1 to 1
- gate_weights: bfloat16 [16, 2048, 512], P('ep', None, 'tp'), may hold values from -0.125 to 0.125
- up_weights: bfloat16 [16, 2048, 512], P('ep', None, 'tp'), may hold values from -0.125 to 0.125
- down_weights: bfloat16 [16, 512, 2048], P('ep', 'tp'), may hold values from -0.25 to 0.25
Outputs:
- updated: bfloat16 [256, 2048], P('ep')
- new_key: bfloat16 [256, 2, 64], P('ep', 'tp')
- new_value: bfloat16 [256, 2, 64], P('ep', 'tp')
- new_logsum: float32 [256, 32], P('ep', 'tp')
The draws below stay inside these ranges and needn't reach their ends.
Inputs may be any that keep to these rules, and one draw needn't show every extreme that they name: `cache_logsum`: non-increasing along the positions. The new token stands at position lengths; some sequence has 1023 cached positions. `expert_ids`: each row names 6 different experts; the rows of one index of ep name one expert at most 12 times.
All inputs are finite; a program needn't handle non-finite values.
Results may differ from the reference program's by a relative error of at most 0.006.
Values may be sent and summed in bfloat16 or wider, within the bound.
No kernel may reach another device: no remote copies, remote signals or barrier semaphores. Data moves between devices by JAX's collectives and lax.ppermute only.
A program may use at most 64 MiB of HBM per device.

```python
import math
import jax
import jax.numpy as jnp
import numpy as np
from jax import lax

D = 2048
HEADS = 32
HD = 64
KV_HEADS = 2
DEXP = 512
TOP_K = 6
CACHE_POSITIONS = 1024
SEQ_DEV = 16
BATCH_SEQUENCES = 256
EXPERTS = 16
CAP = 12
N_EP = 16
N_TP = 2


def draw_cache_keys(key, part):
    random_subkeys = jax.random.split(key, 1)
    values_drawn = jnp.clip(jax.random.normal(random_subkeys[0], (BATCH_SEQUENCES, KV_HEADS, HD, CACHE_POSITIONS), jnp.float32), -6.0, 6.0)
    return values_drawn.astype(jnp.bfloat16)


def draw_cache_logsum(key, part):
    random_subkeys = jax.random.split(key, 7)
    head_order = jax.random.permutation(random_subkeys[0], HEADS)
    is_sluggish = head_order < HEADS // 2
    is_sluggish = is_sluggish.astype(jnp.float32)[None, :, None]
    slow_rate = jax.random.uniform(random_subkeys[1], (1, HEADS, 1), jnp.float32, 0.2, 0.8) / CACHE_POSITIONS
    fast_rate = 1.0 / jax.random.uniform(random_subkeys[2], (1, HEADS, 1), jnp.float32, 30.0, 100.0)
    decay_rate = is_sluggish * slow_rate + (1.0 - is_sluggish) * fast_rate
    sequence_factor = jnp.exp(jax.random.uniform(random_subkeys[3], (BATCH_SEQUENCES, 1, 1), jnp.float32, math.log(0.5), math.log(2.0)))
    random_wobble = jax.random.uniform(random_subkeys[4], (BATCH_SEQUENCES, HEADS, CACHE_POSITIONS), jnp.float32, 0.4, 1.6)
    spike_mask = (jax.random.uniform(random_subkeys[5], (BATCH_SEQUENCES, 1, CACHE_POSITIONS)) < 3.0 / CACHE_POSITIONS).astype(jnp.float32)
    shift_amount = jax.random.uniform(random_subkeys[6], (BATCH_SEQUENCES, HEADS, CACHE_POSITIONS), jnp.float32, 0.22, 0.69)
    step_logarithm = -(decay_rate * sequence_factor * random_wobble) - spike_mask * shift_amount * is_sluggish
    return jnp.cumsum(step_logarithm, axis=-1).astype(jnp.float32)


def draw_lengths(key, part):
    random_subkeys = jax.random.split(key, 2)
    groups = BATCH_SEQUENCES // SEQ_DEV
    device_top = jax.random.randint(random_subkeys[0], (groups, 1), CACHE_POSITIONS // 8, CACHE_POSITIONS - 1)
    raw_bits = jax.random.randint(random_subkeys[1], (groups, SEQ_DEV), 0, 1 << 20)
    lengths_drawn = 2 + raw_bits % (device_top - 1)
    lengths_drawn = lengths_drawn.reshape(BATCH_SEQUENCES).at[0].set(CACHE_POSITIONS - 1)
    return lengths_drawn.astype(jnp.int32)


def levels(own_key, dims, pieces, smallest, high):
    level, own = 1.0, jax.random.fold_in(own_key, 6)
    for position, blocks in pieces:
        steps = jnp.exp(jax.random.uniform(jax.random.fold_in(own, position), (blocks,), jnp.float32, smallest / len(pieces), high / len(pieces)))
        level = level * jnp.repeat(steps, dims[position] // blocks).reshape([-1 if axis == position else 1 for axis in range(len(dims))])
    return level


def deal_out(key, own, number, rows, number_of, top, most, lean):
    sequence = jax.random.permutation(key, number_of)
    packed, ordinary = load_shares(number_of, rows * top, most, lean, True), load_shares(number_of, rows * top, most, lean, False)
    places = jnp.arange(number_of)

    def named(tallies, turn):
        used = int((tallies > 0).sum())
        fixed = max(1, used // 4)
        moved = fixed + (places - fixed + turn * (used - fixed)) % max(1, number_of - fixed)
        return jnp.zeros((number_of,), jnp.int32).at[sequence[jnp.where(places < fixed, places, moved)]].set(jnp.asarray(tallies, jnp.int32))

    tallies = jnp.where(number % 4 == 0, named(packed, number // 4), named(ordinary, number - number // 4 - 1))
    mixed = jax.random.permutation(jax.random.fold_in(own, 3), number_of)
    donor, receiver = mixed[0:number_of // 2 * 2:2], mixed[1:number_of // 2 * 2:2]
    room = jnp.minimum(tallies[donor] - 1, most - tallies[receiver]) // 2
    room = jnp.where((donor == sequence[0]) | (receiver == sequence[0]) | (tallies[receiver] == 0), 0, jnp.maximum(room, 0))
    moved = jax.random.randint(jax.random.fold_in(own, 4), (number_of // 2,), 0, 1 << 20) % (room + 1)
    tallies = tallies.at[donor].add(-moved).at[receiver].add(moved)
    items = jnp.searchsorted(jnp.cumsum(tallies), jnp.arange(rows * top), side="right").astype(jnp.int32)
    listing = items.reshape(top, rows).T
    listing = listing[jax.random.permutation(jax.random.fold_in(own, 1), rows)]
    turn = jax.random.randint(jax.random.fold_in(own, 2), (rows, 1), 0, top)
    return jnp.take_along_axis(listing, (jnp.arange(top)[None, :] + turn) % top, axis=1)


def load_shares(amount, total, reach, skew, full):
    portions = [(1 << 20) // math.isqrt(standing ** skew) + 1 for standing in range(1, amount + 1)]
    largest = reach if full else min(reach, max(-(-total // amount), total * portions[0] // sum(portions)))
    least = 1 if total - largest >= amount - 1 else 0
    given, rest = [largest] + [least] * (amount - 1), total - largest - least * (amount - 1)
    while rest > 0:
        movable = [i for i in range(1, amount) if given[i] < largest] or [i for i in range(1, amount) if given[i] < reach]
        whole, remaining = sum([portions[i] for i in movable]), rest
        for i in movable:
            more = min(reach - given[i], max(1, remaining * portions[i] // whole), rest)
            given[i] = given[i] + more
            rest = rest - more
    return np.array(given)


def bell_draw(stream_key, dims, spread, reach, cuts=(), kind=jnp.bfloat16):
    values = jax.random.normal(stream_key, dims, jnp.float32) * spread
    if len(cuts) > 0:
        values = levels(stream_key, dims, cuts, -0.22, 0.18) * values
    return jnp.clip(values, min=-reach, max=reach).astype(kind)


def setup_inputs(seed: int = 0) -> dict:
    arg_keys = jax.random.split(jax.random.key(seed), 19)
    hidden = bell_draw(arg_keys[0], (BATCH_SEQUENCES, D), 1.0, 6.0, ((0, 16),))
    attn_gain = jnp.clip(1.0 + 0.18 * jax.random.normal(arg_keys[1], (D,), jnp.float32), 0.099609375, 1.8984375).astype(jnp.bfloat16)
    query_weight = bell_draw(arg_keys[2], (D, HEADS * HD), D ** -0.5, 0.125, ((1, 2),))
    key_weight = bell_draw(arg_keys[3], (D, KV_HEADS * HD), D ** -0.5, 0.125, ((1, 2),))
    value_weight = bell_draw(arg_keys[4], (D, KV_HEADS * HD), D ** -0.5, 0.125, ((1, 2),))
    forget_weight = bell_draw(arg_keys[5], (D, HEADS), D ** -0.5, 0.125, ((1, 2),))
    forget_bias = jnp.clip(-1.0 + 5.0 * jax.random.uniform(arg_keys[6], (HEADS,), jnp.float32) ** levels(arg_keys[6], (HEADS,), ((0, 2),), -0.2, 0.2), -1.0, 4.0)
    cache_keys = draw_cache_keys(jax.random.fold_in(arg_keys[18], 71), 0)
    cache_values = bell_draw(arg_keys[8], (BATCH_SEQUENCES, KV_HEADS, HD, CACHE_POSITIONS), 1.0, 6.0, ((0, 16), (1, 2)))
    cache_logsum = draw_cache_logsum(jax.random.fold_in(arg_keys[18], 71), 0)
    lengths = draw_lengths(jax.random.fold_in(arg_keys[18], 71), 0)
    out_weight = bell_draw(arg_keys[11], (D, HEADS * HD), (HEADS * HD) ** -0.5, 0.125, ((0, 16),))
    ffn_gain = jnp.clip(1.0 + 0.18 * jax.random.normal(arg_keys[12], (D,), jnp.float32), 0.099609375, 1.8984375).astype(jnp.bfloat16)
    expert_ids_keys = jax.random.split(jax.random.fold_in(arg_keys[13], 1), BATCH_SEQUENCES // SEQ_DEV)
    expert_ids_turns = jax.random.permutation(jax.random.fold_in(arg_keys[13], 3), BATCH_SEQUENCES // SEQ_DEV)
    expert_ids = jax.vmap(lambda own, number: deal_out(jax.random.fold_in(arg_keys[13], 2), own, number, SEQ_DEV, EXPERTS, TOP_K, CAP, 2))(expert_ids_keys, expert_ids_turns).reshape((BATCH_SEQUENCES, TOP_K))
    expert_scores = jnp.clip(jnp.exp(math.log(1.0) - 2.3025851 * jax.random.uniform(arg_keys[14], (BATCH_SEQUENCES, TOP_K), jnp.float32) ** levels(arg_keys[14], (BATCH_SEQUENCES, TOP_K), ((0, 16),), -0.2, 0.2)), 0.1, 1.0)
    gate_weights = bell_draw(arg_keys[15], (EXPERTS, D, DEXP), D ** -0.5, 0.125, ((0, 16), (2, 2)))
    up_weights = bell_draw(arg_keys[16], (EXPERTS, D, DEXP), D ** -0.5, 0.125, ((0, 16), (2, 2)))
    down_weights = bell_draw(arg_keys[17], (EXPERTS, DEXP, D), DEXP ** -0.5, 0.25, ((0, 16), (1, 2)))
    return {"hidden": hidden, "attn_gain": attn_gain, "query_weight": query_weight, "key_weight": key_weight, "value_weight": value_weight, "forget_weight": forget_weight, "forget_bias": forget_bias, "cache_keys": cache_keys, "cache_values": cache_values, "cache_logsum": cache_logsum, "lengths": lengths, "out_weight": out_weight, "ffn_gain": ffn_gain, "expert_ids": expert_ids, "expert_scores": expert_scores, "gate_weights": gate_weights, "up_weights": up_weights, "down_weights": down_weights}


epsilon = 1e-06

def root_norm(values_in, gain):
    floats = values_in.astype(jnp.float32)
    inv_root = lax.rsqrt(lax.optimization_barrier(jnp.mean(floats * floats, axis=-1, keepdims=True)) + epsilon)
    return floats * inv_root * gain.astype(jnp.float32)

def attend(block):
    queries, keys_block, values_block, logsum_block, lengths_block, key_new, value_new, newsum = block
    rows_here = queries.shape[0]
    query_heads = queries.shape[1] // HD
    key_heads = keys_block.shape[1]
    group_size = query_heads // key_heads
    score_scale = HD ** (-0.5)
    grouped = queries.astype(jnp.float32).reshape(rows_here, key_heads, group_size, HD)
    scores = jnp.einsum('sgjd,sgdp->sgjp', grouped, keys_block.astype(jnp.float32))
    scores = scores.reshape(rows_here, query_heads, CACHE_POSITIONS) * score_scale
    scores = scores + newsum[:, :, None] - logsum_block
    positions = jnp.arange(CACHE_POSITIONS, dtype=jnp.int32)
    is_live = positions[None, :] < lengths_block[:, None]
    scores = jnp.where(is_live[:, None, :], scores, -jnp.inf)
    own_score = jnp.einsum('sgjd,sgd->sgj', grouped, key_new.astype(jnp.float32)).reshape(rows_here, query_heads) * score_scale
    top_score = jnp.maximum(lax.optimization_barrier(jnp.max(scores, axis=-1)), own_score)
    past_exp = jnp.exp(scores - top_score[:, :, None])
    own_exp = jnp.exp(own_score - top_score)
    denominator = lax.optimization_barrier(jnp.sum(past_exp, axis=-1)) + own_exp
    past_weight = (past_exp / denominator[:, :, None]).astype(jnp.bfloat16)
    own_weight = (own_exp / denominator).astype(jnp.bfloat16)
    attended = jnp.einsum('sgjp,sgdp->sgjd', past_weight.astype(jnp.float32).reshape(rows_here, key_heads, group_size, CACHE_POSITIONS), values_block.astype(jnp.float32))
    attended = attended + own_weight.astype(jnp.float32).reshape(rows_here, key_heads, group_size)[:, :, :, None] * value_new.astype(jnp.float32)[:, :, None, :]
    return attended.reshape(rows_here, query_heads * HD).astype(jnp.bfloat16)

def blocked(array):
    return array.reshape((BATCH_SEQUENCES // SEQ_DEV, SEQ_DEV) + array.shape[1:])

def reference(hidden, attn_gain, query_weight, key_weight, value_weight, forget_weight, forget_bias, cache_keys, cache_values, cache_logsum, lengths, out_weight, ffn_gain, expert_ids, expert_scores, gate_weights, up_weights, down_weights):
    normed = root_norm(hidden, attn_gain).astype(jnp.bfloat16)
    queries = jnp.dot(normed, query_weight, preferred_element_type=jnp.float32).astype(jnp.bfloat16)
    new_key = jnp.dot(normed, key_weight, preferred_element_type=jnp.float32).astype(jnp.bfloat16).reshape(BATCH_SEQUENCES, KV_HEADS, HD)
    new_value = jnp.dot(normed, value_weight, preferred_element_type=jnp.float32).astype(jnp.bfloat16).reshape(BATCH_SEQUENCES, KV_HEADS, HD)
    log_forget = jax.nn.log_sigmoid(jnp.dot(normed, forget_weight, preferred_element_type=jnp.float32) + forget_bias)
    positions = jnp.arange(CACHE_POSITIONS, dtype=jnp.int32)
    is_last = positions[None, :] == (lengths - 1)[:, None]
    new_logsum = lax.optimization_barrier(jnp.sum(jnp.where(is_last[:, None, :], cache_logsum, 0.0), axis=-1)) + log_forget
    blocks = tuple((blocked(array) for array in (queries, cache_keys, cache_values, cache_logsum, lengths, new_key, new_value, new_logsum)))
    attended = lax.map(attend, blocks).reshape(BATCH_SEQUENCES, HEADS * HD)
    mixed = jnp.dot(attended, out_weight.T, preferred_element_type=jnp.float32).astype(jnp.bfloat16)
    residual = hidden.astype(jnp.float32) + mixed.astype(jnp.float32)
    ffn_in = root_norm(residual, ffn_gain).astype(jnp.bfloat16)
    route_count = BATCH_SEQUENCES * TOP_K
    flat_ids = expert_ids.reshape(route_count)
    onehot = (flat_ids[:, None] == jnp.arange(EXPERTS, dtype=jnp.int32)[None, :]).astype(jnp.int32)
    running = jnp.cumsum(onehot.reshape(N_EP, SEQ_DEV * TOP_K, EXPERTS), axis=1).reshape(route_count, EXPERTS)
    slot_index = lax.optimization_barrier(jnp.sum(running * onehot, axis=1)) - 1
    source = jnp.arange(route_count, dtype=jnp.int32) // (SEQ_DEV * TOP_K)
    placement = flat_ids * (N_EP * CAP) + source * CAP + slot_index
    token_of_route = jnp.arange(route_count, dtype=jnp.int32) // TOP_K
    slot_table = jnp.full((EXPERTS * N_EP * CAP,), BATCH_SEQUENCES, dtype=jnp.int32).at[placement].set(token_of_route)
    padded = jnp.concatenate([ffn_in, jnp.zeros((1, D), jnp.bfloat16)], axis=0)
    expert_rows = padded[slot_table].reshape(EXPERTS, N_EP * CAP, D)
    share_width = DEXP // N_TP

    def run_expert(block):
        rows_in, gate_one, up_one, down_one = block
        gate_act = jnp.dot(rows_in, gate_one, preferred_element_type=jnp.float32)
        up_act = jnp.dot(rows_in, up_one, preferred_element_type=jnp.float32)
        hidden_act = (jax.nn.silu(gate_act) * up_act).astype(jnp.bfloat16)
        summed = jnp.zeros((rows_in.shape[0], D), jnp.float32)
        for block_index in range(N_TP):
            lower = block_index * share_width
            partial_value = jnp.dot(hidden_act[:, lower:lower + share_width], down_one[lower:lower + share_width], preferred_element_type=jnp.float32)
            summed = summed + partial_value.astype(jnp.bfloat16).astype(jnp.float32)
        return summed.astype(jnp.bfloat16)
    expert_outputs = lax.map(run_expert, (expert_rows, gate_weights, up_weights, down_weights))
    route_out = expert_outputs.reshape(EXPERTS * N_EP * CAP, D)[placement].astype(jnp.float32).reshape(BATCH_SEQUENCES, TOP_K, D)
    route_weight = expert_scores / lax.optimization_barrier(jnp.sum(expert_scores, axis=-1, keepdims=True))
    updated = (residual + lax.optimization_barrier(jnp.sum(route_out * route_weight[:, :, None], axis=1))).astype(jnp.bfloat16)
    return (updated, new_key, new_value, new_logsum)
```

```python
import jax
import jax.numpy as jnp
from jax import lax
from jax.sharding import PartitionSpec as P

HD = 64

epsilon = 1e-06
SWAP = ((0, 1), (1, 0))


def root_norm(values_in, gain):
    floats = values_in.astype(jnp.float32)
    inv_root = lax.rsqrt(jnp.mean(floats * floats, axis=-1, keepdims=True) + epsilon)
    return floats * inv_root * gain.astype(jnp.float32)


def attention(
    hidden,
    attn_gain,
    query_weight,
    key_weight,
    value_weight,
    forget_weight,
    forget_bias,
    cache_keys,
    cache_values,
    cache_logsum,
    lengths,
):
    rows_here = hidden.shape[0]
    query_heads = query_weight.shape[1] // HD
    key_heads = key_weight.shape[1] // HD
    group_size = query_heads // key_heads
    cache_len = cache_keys.shape[-1]
    score_scale = HD ** (-0.5)
    normed = root_norm(hidden, attn_gain).astype(jnp.bfloat16)
    queries = jnp.dot(normed, query_weight, preferred_element_type=jnp.float32).astype(jnp.bfloat16)
    key_new = (
        jnp.dot(normed, key_weight, preferred_element_type=jnp.float32)
        .astype(jnp.bfloat16)
        .reshape(rows_here, key_heads, HD)
    )
    value_new = (
        jnp.dot(normed, value_weight, preferred_element_type=jnp.float32)
        .astype(jnp.bfloat16)
        .reshape(rows_here, key_heads, HD)
    )
    log_forget = jax.nn.log_sigmoid(
        jnp.dot(normed, forget_weight, preferred_element_type=jnp.float32) + forget_bias
    )
    positions = jnp.arange(cache_len, dtype=jnp.int32)
    is_last = positions[None, :] == (lengths - 1)[:, None]
    new_logsum = jnp.sum(jnp.where(is_last[:, None, :], cache_logsum, 0.0), axis=-1) + log_forget
    grouped = queries.reshape(rows_here, key_heads, group_size, HD)
    scores = jnp.einsum("sgjd,sgdp->sgjp", grouped, cache_keys, preferred_element_type=jnp.float32)
    scores = scores.reshape(rows_here, query_heads, cache_len) * score_scale
    scores = scores + new_logsum[:, :, None] - cache_logsum
    is_live = positions[None, :] < lengths[:, None]
    scores = jnp.where(is_live[:, None, :], scores, -jnp.inf)
    own_score = (
        jnp.einsum("sgjd,sgd->sgj", grouped, key_new, preferred_element_type=jnp.float32).reshape(
            rows_here, query_heads
        )
        * score_scale
    )
    top_score = jnp.maximum(jnp.max(scores, axis=-1), own_score)
    past_exp = jnp.exp(scores - top_score[:, :, None])
    own_exp = jnp.exp(own_score - top_score)
    denominator = jnp.sum(past_exp, axis=-1) + own_exp
    past_weight = (past_exp / denominator[:, :, None]).astype(jnp.bfloat16)
    own_weight = (own_exp / denominator).astype(jnp.bfloat16)
    attended = jnp.einsum(
        "sgjp,sgdp->sgjd",
        past_weight.reshape(rows_here, key_heads, group_size, cache_len),
        cache_values,
        preferred_element_type=jnp.float32,
    )
    attended = (
        attended
        + own_weight.astype(jnp.float32).reshape(rows_here, key_heads, group_size)[:, :, :, None]
        * value_new.astype(jnp.float32)[:, :, None, :]
    )
    attended = attended.reshape(rows_here, query_heads * HD).astype(jnp.bfloat16)
    return attended, key_new, value_new, new_logsum


def per_device(
    hidden,
    attn_gain,
    query_weight,
    key_weight,
    value_weight,
    forget_weight,
    forget_bias,
    cache_keys,
    cache_values,
    cache_logsum,
    lengths,
    out_weight,
    ffn_gain,
    expert_ids,
    expert_scores,
    gate_weights,
    up_weights,
    down_weights,
):
    f32, bf16 = jnp.float32, jnp.bfloat16
    rows_here, width = hidden.shape
    ep_size, tp_size = lax.axis_size("ep"), lax.axis_size("tp")
    ep_index, tp_index = lax.axis_index("ep"), lax.axis_index("tp")
    half = rows_here // tp_size
    slice_width = out_weight.shape[0]
    local_experts = gate_weights.shape[0]

    gate_other = lax.ppermute(gate_weights, "tp", SWAP)
    up_other = lax.ppermute(up_weights, "tp", SWAP)
    down_other = lax.ppermute(down_weights, "tp", SWAP)

    attended, key_new, value_new, new_logsum = attention(
        hidden,
        attn_gain,
        query_weight,
        key_weight,
        value_weight,
        forget_weight,
        forget_bias,
        cache_keys,
        cache_values,
        cache_logsum,
        lengths,
    )

    is_first = tp_index == 0
    low, high = attended[:half], attended[half:]
    mine = jnp.where(is_first, low, high)
    theirs = lax.ppermute(jnp.where(is_first, high, low), "tp", SWAP)
    whole = jnp.concatenate(
        [jnp.where(is_first, mine, theirs), jnp.where(is_first, theirs, mine)], axis=1
    )
    hidden_mine = jnp.where(is_first, hidden[:half], hidden[half:])

    hidden_parts = jnp.swapaxes(hidden_mine.reshape(half, ep_size, slice_width), 0, 1)
    outgoing = jnp.concatenate(
        [jnp.broadcast_to(whole[None], (ep_size,) + whole.shape), hidden_parts], axis=2
    )
    arrived = lax.all_to_all(outgoing, "ep", split_axis=0, concat_axis=0, tiled=True)
    arrived = arrived.reshape(ep_size * half, whole.shape[1] + slice_width)
    mixed = lax.dot_general(
        arrived[:, : whole.shape[1]],
        out_weight,
        (((1,), (1,)), ((), ())),
        preferred_element_type=f32,
    ).astype(bf16)
    residual_part = (arrived[:, whole.shape[1] :].astype(f32) + mixed.astype(f32)).astype(bf16)

    blocks = lax.all_to_all(
        jnp.broadcast_to(residual_part[None], (ep_size,) + residual_part.shape),
        "ep",
        split_axis=0,
        concat_axis=0,
        tiled=True,
    )
    residual = jnp.swapaxes(blocks, 0, 1).reshape(ep_size * half, width)
    ffn_in = root_norm(residual, ffn_gain).astype(bf16)

    outs = []
    for expert in range(local_experts):
        total = jnp.zeros((), f32)
        for gate, up, down in (
            (gate_weights, up_weights, down_weights),
            (gate_other, up_other, down_other),
        ):
            gate_act = jnp.dot(ffn_in, gate[expert], preferred_element_type=f32)
            up_act = jnp.dot(ffn_in, up[expert], preferred_element_type=f32)
            hidden_act = (jax.nn.silu(gate_act) * up_act).astype(bf16)
            total = total + jnp.dot(hidden_act, down[expert], preferred_element_type=f32)
        outs.append(total.astype(bf16).reshape(ep_size, half, 1, width))
    returned = lax.all_to_all(
        jnp.concatenate(outs, axis=2) if local_experts > 1 else outs[0][:, :, 0],
        "ep",
        split_axis=0,
        concat_axis=0,
        tiled=True,
    ).reshape(ep_size, half, local_experts, width)

    experts = ep_size * local_experts
    route_weight = expert_scores / jnp.sum(expert_scores, axis=-1, keepdims=True)
    chosen = expert_ids[:, :, None] == jnp.arange(experts, dtype=jnp.int32)
    expert_weight = jnp.sum(jnp.where(chosen, route_weight[:, :, None], 0.0), axis=1)
    weight_mine = jnp.where(is_first, expert_weight[:half], expert_weight[half:])
    weight_mine = jnp.swapaxes(weight_mine.reshape(half, ep_size, local_experts), 0, 1)
    expert_mix = jnp.sum(returned.astype(f32) * weight_mine[:, :, :, None], axis=(0, 2))
    own = lax.dynamic_slice_in_dim(residual, ep_index * half, half, 0)
    updated_mine = (own.astype(f32) + expert_mix).astype(bf16)
    updated_theirs = lax.ppermute(updated_mine, "tp", SWAP)
    updated = jnp.concatenate(
        [
            jnp.where(is_first, updated_mine, updated_theirs),
            jnp.where(is_first, updated_theirs, updated_mine),
        ],
        axis=0,
    )
    return (updated, key_new, value_new, new_logsum)
def solution(mesh):
    in_specs = (
        P("ep", None),
        P(),
        P(None, "tp"),
        P(None, "tp"),
        P(None, "tp"),
        P(None, "tp"),
        P("tp"),
        P("ep", "tp", None, None),
        P("ep", "tp", None, None),
        P("ep", "tp", None),
        P("ep"),
        P("ep", None),
        P(),
        P("ep", None),
        P("ep", None),
        P("ep", None, "tp"),
        P("ep", None, "tp"),
        P("ep", "tp", None),
    )
    out_specs = (P("ep", None), P("ep", "tp", None), P("ep", "tp", None), P("ep", "tp"))
    return jax.shard_map(
        per_device, mesh=mesh, in_specs=in_specs, out_specs=out_specs, check_vma=False
    )
```

```python
import functools

import jax
import jax.numpy as jnp
from jax import lax
from jax.experimental import pallas as pl
from jax.experimental.pallas import tpu as pltpu
from jax.sharding import PartitionSpec as P

HD = 64
GROUPS = 4
VMEM_LIMIT = 24 * 1024 * 1024

epsilon = 1e-06
SWAP = ((0, 1), (1, 0))


def attention_kernel(
    lengths_ref, hidden_ref, gain_ref, query_ref, key_ref, value_ref, forget_ref, bias_ref,
    keys_ref, values_ref, logsum_ref,
    *refs,
):
    (
        *payload_refs, new_key_ref, new_value_ref, new_logsum_ref,
        hidden_buf, gain_buf, query_buf, key_buf, value_buf, forget_buf, bias_buf,
        keys_buf, values_buf, logsum_buf, queries_buf, heads_buf, slices_buf, sems,
    ) = refs
    f32, bf16 = jnp.float32, jnp.bfloat16
    rows, width = hidden_buf.shape
    heads = forget_buf.shape[0]
    cache_len = keys_buf.shape[-1]
    count = [0]

    def fetch(source, target):
        copy = pltpu.make_async_copy(source, target, sems.at[count[0]])
        count[0] += 1
        copy.start()
        return copy

    small = [
        fetch(a, b)
        for a, b in (
            (hidden_ref, hidden_buf),
            (gain_ref, gain_buf),
            (bias_ref, bias_buf),
            (forget_ref, forget_buf),
            (key_ref, key_buf),
            (value_ref, value_buf),
        )
    ]
    parts = 4
    depth = width // parts
    query_copies = [
        fetch(query_ref.at[pl.ds(i * depth, depth)], query_buf.at[pl.ds(i * depth, depth)])
        for i in range(parts)
    ]
    group = rows // GROUPS
    past = []
    for i in range(GROUPS):
        at = pl.ds(i * group, group)
        past.append(
            [
                fetch(a.at[at], b.at[at])
                for a, b in (
                    (logsum_ref, logsum_buf), (keys_ref, keys_buf), (values_ref, values_buf)
                )
            ]
        )

    for copy in small:
        copy.wait()
    floats = hidden_buf[...].astype(f32)
    inv_root = lax.rsqrt(jnp.mean(floats * floats, axis=-1, keepdims=True) + epsilon)
    normed = (floats * inv_root * gain_buf[...].astype(f32).reshape(1, width)).astype(bf16)
    across = (((1,), (1,)), ((), ()))
    new_key = lax.dot_general(normed, key_buf[...], across, preferred_element_type=f32).astype(bf16)
    new_value = lax.dot_general(normed, value_buf[...], across, preferred_element_type=f32).astype(bf16)
    new_key_ref[...] = new_key
    new_value_ref[...] = new_value
    logits = lax.dot_general(normed, forget_buf[...], across, preferred_element_type=f32) + bias_buf[...]
    log_forget = jnp.minimum(logits, 0.0) - jnp.log1p(jnp.exp(-jnp.abs(logits)))
    turn = functools.partial(
        lax.dot_general, dimension_numbers=across, preferred_element_type=f32,
        precision=lax.Precision.HIGHEST,
    )

    def eye(size):
        return (
            lax.broadcasted_iota(jnp.int32, (size, size), 0)
            == lax.broadcasted_iota(jnp.int32, (size, size), 1)
        ).astype(f32)

    log_forget = turn(eye(heads), log_forget)
    queries = jnp.zeros((rows, heads * HD), f32)
    for i, copy in enumerate(query_copies):
        copy.wait()
        at = slice(i * depth, (i + 1) * depth)
        queries = queries + jnp.dot(normed[:, at], query_buf[at, :], preferred_element_type=f32)
    queries = queries.astype(bf16).astype(f32) * HD ** (-0.5)
    for h in range(heads):
        queries_buf[pl.ds(h * rows, rows), :] = queries[:, h * HD : (h + 1) * HD]
    new_key_f, new_value_f = new_key.astype(f32), new_value.astype(f32)
    lane = lax.broadcasted_iota(jnp.int32, (heads, 128), 1)
    position = lax.broadcasted_iota(jnp.int32, (heads, cache_len), 1)
    column = lax.broadcasted_iota(jnp.int32, (heads, rows), 1)
    collected = jnp.zeros((heads, rows), f32)
    for s in range(rows):
        if s % group == 0:
            for copy in past[s // group]:
                copy.wait()
        length = lengths_ref[s]
        query = queries_buf[pl.ds(s, heads, stride=rows), :]
        base = pl.multiple_of((length - 1) // 128 * 128, 128)
        last = logsum_buf[s, :, pl.ds(base, 128)]
        last = jnp.sum(jnp.where(lane == length - 1 - base, last, 0.0), axis=-1, keepdims=True)
        newest = last + log_forget[:, s : s + 1]
        collected = jnp.where(column == s, newest, collected)
        scores = jnp.dot(query.astype(bf16), keys_buf[s], preferred_element_type=f32)
        scores = scores + (newest - logsum_buf[s])
        scores = jnp.where(position < length, scores, -jnp.inf)
        own = jnp.sum(query * new_key_f[s : s + 1, :], axis=-1, keepdims=True)
        top = jnp.maximum(jnp.max(scores, axis=-1, keepdims=True), own)
        weight = jnp.exp(scores - top)
        own_weight = jnp.exp(own - top)
        total = jnp.sum(weight, axis=-1, keepdims=True) + own_weight
        out = lax.dot_general(weight.astype(bf16), values_buf[s], across, preferred_element_type=f32)
        out = (out + own_weight * new_value_f[s : s + 1, :]) / total
        heads_buf[pl.ds(s, heads, stride=rows), :] = out
    new_logsum_ref[...] = turn(eye(rows), collected)
    for h in range(0, heads, 2):
        pair = jnp.concatenate(
            [heads_buf[pl.ds(h * rows, rows), :], heads_buf[pl.ds((h + 1) * rows, rows), :]], axis=1
        )
        for payload_ref in payload_refs:
            payload_ref[:rows, h * HD : (h + 2) * HD] = pair.astype(bf16)
    outer, half, part = slices_buf.shape
    is_first = lax.axis_index("tp") == 0
    for i in range(outer):
        at = slice(i * part, (i + 1) * part)
        slices_buf[i] = jnp.where(is_first, hidden_buf[:half, at], hidden_buf[half:, at])
    place = lax.axis_index("ep") // (lax.axis_size("ep") // outer)
    for i, payload_ref in enumerate(payload_refs):
        payload_ref[rows:, :part] = slices_buf[place ^ i]
        if part < payload_ref.shape[1]:
            payload_ref[rows:, part:] = jnp.zeros((half, payload_ref.shape[1] - part), bf16)


def attention(
    hidden, attn_gain, query_weight, key_weight, value_weight, forget_weight, forget_bias,
    cache_keys, cache_values, cache_logsum, lengths, outer,
):
    f32, bf16 = jnp.float32, jnp.bfloat16
    rows, width = hidden.shape
    half = rows // lax.axis_size("tp")
    heads = forget_weight.shape[1]
    cache_len = cache_keys.shape[-1]
    any_spec = pl.BlockSpec(memory_space=pl.ANY)
    args = (
        lengths, hidden, attn_gain, query_weight, key_weight.T, value_weight.T, forget_weight.T,
        forget_bias[None], cache_keys[:, 0], cache_values[:, 0], cache_logsum,
    )
    vmem = pl.BlockSpec(memory_space=pltpu.VMEM)
    bytes_read = sum(a.size * a.dtype.itemsize for a in args)
    *payloads, new_key, new_value, new_logsum = pl.pallas_call(
        attention_kernel,
        out_shape=(
            *(jax.ShapeDtypeStruct((rows + half, heads * HD), bf16),) * outer,
            jax.ShapeDtypeStruct((rows, HD), bf16),
            jax.ShapeDtypeStruct((rows, HD), bf16),
            jax.ShapeDtypeStruct((rows, heads), f32),
        ),
        in_specs=[pl.BlockSpec(memory_space=pltpu.SMEM)] + [any_spec] * 10,
        out_specs=(vmem,) * (outer + 3),
        scratch_shapes=[pltpu.VMEM(a.shape, a.dtype) for a in args[1:]]
        + [
            pltpu.VMEM((heads * rows, HD), f32),
            pltpu.VMEM((heads * rows, HD), f32),
            pltpu.VMEM((outer, half, width // outer), bf16),
            pltpu.SemaphoreType.DMA((10 + 3 * GROUPS,)),
        ],
        compiler_params=pltpu.CompilerParams(vmem_limit_bytes=60 * 1024 * 1024),
        cost_estimate=pl.CostEstimate(
            flops=2 * rows * heads * HD * (width + 2 * cache_len),
            bytes_accessed=bytes_read,
            transcendentals=rows * heads * cache_len,
        ),
        name="attention",
    )(*args)
    return payloads, new_key[:, None], new_value[:, None], new_logsum


def project_kernel(outer, inner, *refs):
    f32 = jnp.float32
    payload_refs, refs = refs[:outer], refs[outer:]
    weight_refs, refs = refs[:inner], refs[inner:]
    keep_ref, send_ref, hidden_ref, rows_buf, sums_buf = refs
    rows = rows_buf.shape[0] // outer
    half = payload_refs[0].shape[0] - rows
    part = hidden_ref.shape[1]
    depth = weight_refs[0].shape[0]
    is_first = lax.axis_index("tp") == 0
    index = lax.axis_index("ep")
    place, line = index // inner, index % inner
    for i, payload_ref in enumerate(payload_refs):
        at = place ^ i
        rows_buf[pl.ds(pl.multiple_of(at * rows, rows), rows), :] = payload_ref[:rows, :]
        hidden_ref[pl.ds(pl.multiple_of(at * half, half), half), :] = payload_ref[rows:, :part]
    for i, weight_ref in enumerate(weight_refs):
        sums_buf[line ^ i] = lax.dot_general(
            rows_buf[...], weight_ref[...], (((1,), (1,)), ((), ())), preferred_element_type=f32
        )
    for i in range(inner):
        lanes = slice(i * depth, (i + 1) * depth)
        for k in range(outer):
            low = sums_buf[i, k * rows : k * rows + half, :]
            high = sums_buf[i, k * rows + half : (k + 1) * rows, :]
            at = slice(k * half, (k + 1) * half)
            keep_ref[at, lanes] = jnp.where(is_first, low, high)
            send_ref[at, lanes] = jnp.where(is_first, high, low)


def project(payloads, weights, half):
    f32, bf16 = jnp.float32, jnp.bfloat16
    outer, inner = len(payloads), len(weights)
    rows = payloads[0].shape[0] - half
    depth, width = weights[0].shape
    vmem = pl.BlockSpec(memory_space=pltpu.VMEM)
    total = jax.ShapeDtypeStruct((outer * half, inner * depth), f32)
    return pl.pallas_call(
        functools.partial(project_kernel, outer, inner),
        out_shape=(total, total, jax.ShapeDtypeStruct(total.shape, bf16)),
        in_specs=[vmem] * (outer + inner),
        out_specs=(vmem,) * 3,
        scratch_shapes=[
            pltpu.VMEM((outer * rows, width), bf16),
            pltpu.VMEM((inner, outer * rows, depth), f32),
        ],
        compiler_params=pltpu.CompilerParams(vmem_limit_bytes=VMEM_LIMIT),
        cost_estimate=pl.CostEstimate(
            flops=2 * outer * rows * width * inner * depth,
            bytes_accessed=2 * (outer * rows + inner * depth) * width,
            transcendentals=0,
        ),
        name="project",
    )(*payloads, *weights)


def experts_kernel(outer, inner, blocks_ref, gain_ref, *refs):
    f32, bf16 = jnp.float32, jnp.bfloat16
    *weights, out_ref, own_ref, inputs_buf = refs
    _, group, part = blocks_ref.shape
    half = group // outer
    width = outer * part
    index = lax.axis_index("ep")
    place, line = index // inner, index % inner
    gain = gain_ref[...].astype(f32).reshape(1, width)
    own_rows = pl.ds(pl.multiple_of(place * half, half), half)
    for z in range(outer):
        lanes = slice(z * part, (z + 1) * part)
        own_ref[:, lanes] = blocks_ref[z * inner + line, own_rows, :]
    for p in range(inner):
        squares = jnp.zeros((group, 1), f32)
        for z in range(outer):
            floats = blocks_ref[z * inner + p].astype(f32)
            squares = squares + jnp.sum(floats * floats, axis=-1, keepdims=True)
        inv_root = lax.rsqrt(squares / width + epsilon)
        for z in range(outer):
            lanes = slice(z * part, (z + 1) * part)
            floats = blocks_ref[z * inner + p].astype(f32)
            inputs_buf[p * group : (p + 1) * group, lanes] = (
                floats * inv_root * gain[:, lanes]
            ).astype(bf16)
    for expert in range(weights[0].shape[0]):
        acts = []
        for gate_ref, up_ref in ((weights[0], weights[1]), (weights[3], weights[4])):
            gate = jnp.dot(inputs_buf[...], gate_ref[expert], preferred_element_type=f32)
            up = jnp.dot(inputs_buf[...], up_ref[expert], preferred_element_type=f32)
            acts.append((gate / (1.0 + jnp.exp(-gate)) * up).astype(bf16))
        total = jnp.dot(acts[0], weights[2][expert], preferred_element_type=f32)
        total = total + jnp.dot(acts[1], weights[5][expert], preferred_element_type=f32)
        for p in range(inner):
            for z in range(outer):
                at = p * group + z * half
                out_ref[z * inner + p, expert] = total[at : at + half].astype(bf16)


def experts(blocks, gain, own, other, outer, inner):
    ep_size, group, part = blocks.shape
    width = outer * part
    half = group // outer
    rows = ep_size * half
    local, _, depth = own[0].shape
    vmem = pl.BlockSpec(memory_space=pltpu.VMEM)
    return pl.pallas_call(
        functools.partial(experts_kernel, outer, inner),
        out_shape=(
            jax.ShapeDtypeStruct((ep_size, local, half, width), jnp.bfloat16),
            jax.ShapeDtypeStruct((half, width), jnp.bfloat16),
        ),
        in_specs=[vmem] * 8,
        out_specs=(vmem,) * 2,
        scratch_shapes=[pltpu.VMEM((rows, width), jnp.bfloat16)],
        compiler_params=pltpu.CompilerParams(vmem_limit_bytes=VMEM_LIMIT),
        cost_estimate=pl.CostEstimate(
            flops=12 * local * rows * width * depth,
            bytes_accessed=2 * (2 * rows * width + 6 * local * width * depth),
            transcendentals=2 * local * rows * depth,
        ),
        name="experts",
    )(blocks, gain, *own, *other)


def over_lines(arrays, inner):
    ep_size, outer = lax.axis_size("ep"), len(arrays)
    if outer <= 4:
        return arrays[:1] + [
            lax.ppermute(a, "ep", [(e, e ^ (i * inner)) for e in range(ep_size)])
            for i, a in list(enumerate(arrays))[1:]
        ]
    place = lax.axis_index("ep") // inner
    order = jnp.arange(outer, dtype=jnp.int32) ^ place
    groups = [[z * inner + p for z in range(outer)] for p in range(inner)]
    moved = lax.all_to_all(
        jnp.stack(arrays)[order], "ep", 0, 0, axis_index_groups=groups, tiled=True
    )
    return list(moved[order])


def per_device(
    hidden,
    attn_gain,
    query_weight,
    key_weight,
    value_weight,
    forget_weight,
    forget_bias,
    cache_keys,
    cache_values,
    cache_logsum,
    lengths,
    out_weight,
    ffn_gain,
    expert_ids,
    expert_scores,
    gate_weights,
    up_weights,
    down_weights,
):
    f32, bf16 = jnp.float32, jnp.bfloat16
    rows_here, width = hidden.shape
    ep_size, tp_size = lax.axis_size("ep"), lax.axis_size("tp")
    tp_index = lax.axis_index("tp")
    is_first = tp_index == 0
    half = rows_here // tp_size
    local_experts = gate_weights.shape[0]

    gate_other = lax.ppermute(gate_weights, "tp", SWAP)
    up_other = lax.ppermute(up_weights, "tp", SWAP)
    down_other = lax.ppermute(down_weights, "tp", SWAP)

    inner = 4 if ep_size % 4 == 0 else 1
    outer = ep_size // inner
    heads_here = query_weight.shape[1]
    with jax.named_scope("share"):
        weight_half = lax.dynamic_slice_in_dim(out_weight, tp_index * heads_here, heads_here, 1)
        shared = [weight_half] + [
            lax.ppermute(weight_half, "ep", [(e, e ^ i) for e in range(ep_size)])
            for i in range(1, inner)
        ]
    with jax.named_scope("attend"):
        payloads, key_new, value_new, new_logsum = attention(
            hidden,
            attn_gain,
            query_weight,
            key_weight,
            value_weight,
            forget_weight,
            forget_bias,
            cache_keys,
            cache_values,
            cache_logsum,
            lengths,
            outer,
        )
    with jax.named_scope("lines"):
        payloads = over_lines(payloads, inner)
    keep, send, hidden_part = project(payloads, shared, half)
    mixed = (keep + lax.ppermute(send, "tp", SWAP)).astype(bf16)
    residual_part = (hidden_part.astype(f32) + mixed.astype(f32)).astype(bf16)

    blocks = lax.all_to_all(
        jnp.broadcast_to(residual_part[None], (ep_size,) + residual_part.shape),
        "ep",
        split_axis=0,
        concat_axis=0,
        tiled=True,
    )
    outgoing, own = experts(
        blocks,
        ffn_gain,
        (gate_weights, up_weights, down_weights),
        (gate_other, up_other, down_other),
        outer,
        inner,
    )
    returned = lax.all_to_all(outgoing, "ep", split_axis=0, concat_axis=0, tiled=True)

    expert_count = ep_size * local_experts
    route_weight = expert_scores / jnp.sum(expert_scores, axis=-1, keepdims=True)
    chosen = expert_ids[:, :, None] == jnp.arange(expert_count, dtype=jnp.int32)
    expert_weight = jnp.sum(jnp.where(chosen, route_weight[:, :, None], 0.0), axis=1)
    weight_mine = jnp.where(is_first, expert_weight[:half], expert_weight[half:])
    weight_mine = weight_mine.T.reshape(ep_size, local_experts, half)
    expert_mix = jnp.sum(returned.astype(f32) * weight_mine[:, :, :, None], axis=(0, 1))
    updated_mine = (own.astype(f32) + expert_mix).astype(bf16)
    updated_theirs = lax.ppermute(updated_mine, "tp", SWAP)
    updated = jnp.concatenate(
        [
            jnp.where(is_first, updated_mine, updated_theirs),
            jnp.where(is_first, updated_theirs, updated_mine),
        ],
        axis=0,
    )
    return (updated, key_new, value_new, new_logsum)
def solution(mesh):
    in_specs = (
        P("ep", None),
        P(),
        P(None, "tp"),
        P(None, "tp"),
        P(None, "tp"),
        P(None, "tp"),
        P("tp"),
        P("ep", "tp", None, None),
        P("ep", "tp", None, None),
        P("ep", "tp", None),
        P("ep"),
        P("ep", None),
        P(),
        P("ep", None),
        P("ep", None),
        P("ep", None, "tp"),
        P("ep", None, "tp"),
        P("ep", "tp", None),
    )
    out_specs = (P("ep", None), P("ep", "tp", None), P("ep", "tp", None), P("ep", "tp"))
    return jax.shard_map(
        per_device, mesh=mesh, in_specs=in_specs, out_specs=out_specs, check_vma=False
    )
```

```python
import functools

import jax
import jax.numpy as jnp
from jax import lax
from jax.experimental import pallas as pl
from jax.experimental.pallas import tpu as pltpu
from jax.sharding import PartitionSpec as P

HD = 64
GROUPS = 2
EXPERTS_LIMIT = 16 * 1024 * 1024
VMEM_LIMIT = 24 * 1024 * 1024

epsilon = 1e-06
SWAP = ((0, 1), (1, 0))


def attention_kernel(
    lengths_ref, hidden_ref, gain_ref, query_ref, key_ref, value_ref, forget_ref, bias_ref,
    keys_ref, values_ref, logsum_ref,
    *refs,
):
    (
        *payload_refs, new_key_ref, new_value_ref, new_logsum_ref,
        hidden_buf, gain_buf, query_buf, key_buf, value_buf, forget_buf, bias_buf,
        keys_buf, values_buf, logsum_buf, queries_buf, heads_buf, slices_buf, sems,
    ) = refs
    f32, bf16 = jnp.float32, jnp.bfloat16
    rows, width = hidden_buf.shape
    heads = forget_buf.shape[0]
    cache_len = keys_buf.shape[-1]
    count = [0]

    def fetch(source, target):
        copy = pltpu.make_async_copy(source, target, sems.at[count[0]])
        count[0] += 1
        copy.start()
        return copy

    small = [
        fetch(a, b)
        for a, b in (
            (hidden_ref, hidden_buf),
            (gain_ref, gain_buf),
            (bias_ref, bias_buf),
            (forget_ref, forget_buf),
            (key_ref, key_buf),
            (value_ref, value_buf),
        )
    ]
    parts = 4
    depth = width // parts
    query_copies = [
        fetch(query_ref.at[pl.ds(i * depth, depth)], query_buf.at[pl.ds(i * depth, depth)])
        for i in range(parts)
    ]
    group = rows // GROUPS
    past = []
    for i in range(GROUPS):
        at = pl.ds(i * group, group)
        past.append(
            [
                fetch(a.at[at], b.at[at])
                for a, b in (
                    (logsum_ref, logsum_buf), (keys_ref, keys_buf), (values_ref, values_buf)
                )
            ]
        )

    for copy in small:
        copy.wait()
    floats = hidden_buf[...].astype(f32)
    inv_root = lax.rsqrt(jnp.mean(floats * floats, axis=-1, keepdims=True) + epsilon)
    normed = (floats * inv_root * gain_buf[...].astype(f32).reshape(1, width)).astype(bf16)
    across = (((1,), (1,)), ((), ()))
    new_key = lax.dot_general(normed, key_buf[...], across, preferred_element_type=f32).astype(bf16)
    new_value = lax.dot_general(normed, value_buf[...], across, preferred_element_type=f32).astype(bf16)
    new_key_ref[...] = new_key
    new_value_ref[...] = new_value
    logits = lax.dot_general(normed, forget_buf[...], across, preferred_element_type=f32) + bias_buf[...]
    log_forget = jnp.minimum(logits, 0.0) - jnp.log1p(jnp.exp(-jnp.abs(logits)))
    turn = functools.partial(
        lax.dot_general, dimension_numbers=across, preferred_element_type=f32,
        precision=lax.Precision.HIGHEST,
    )

    def eye(size):
        return (
            lax.broadcasted_iota(jnp.int32, (size, size), 0)
            == lax.broadcasted_iota(jnp.int32, (size, size), 1)
        ).astype(f32)

    log_forget = turn(eye(heads), log_forget)
    queries = jnp.zeros((rows, heads * HD), f32)
    for i, copy in enumerate(query_copies):
        copy.wait()
        at = slice(i * depth, (i + 1) * depth)
        queries = queries + jnp.dot(normed[:, at], query_buf[at, :], preferred_element_type=f32)
    queries = queries.astype(bf16).astype(f32) * HD ** (-0.5)
    for h in range(heads):
        queries_buf[pl.ds(h * rows, rows), :] = queries[:, h * HD : (h + 1) * HD]
    new_key_f, new_value_f = new_key.astype(f32), new_value.astype(f32)
    lane = lax.broadcasted_iota(jnp.int32, (heads, 128), 1)
    position = lax.broadcasted_iota(jnp.int32, (heads, cache_len), 1)
    column = lax.broadcasted_iota(jnp.int32, (heads, rows), 1)
    collected = jnp.zeros((heads, rows), f32)
    for first in range(0, rows, group):
        for copy in past[first // group]:
            copy.wait()
        members = range(first, first + group)
        query = {s: queries_buf[pl.ds(s, heads, stride=rows), :] for s in members}
        dots = {
            s: jnp.dot(query[s].astype(bf16), keys_buf[s], preferred_element_type=f32)
            for s in members
        }
        newest, own = {}, {}
        for s in members:
            last_at = lengths_ref[s] - 1
            base = pl.multiple_of(last_at // 128 * 128, 128)
            last = logsum_buf[s, :, pl.ds(base, 128)]
            last = jnp.where(lane == last_at - base, last, 0.0)
            newest[s] = jnp.sum(last, axis=-1, keepdims=True) + log_forget[:, s : s + 1]
            own[s] = jnp.sum(query[s] * new_key_f[s : s + 1, :], axis=-1, keepdims=True)
        for s in members:
            collected = jnp.where(column == s, newest[s], collected)
            scores = dots[s] + (newest[s] - logsum_buf[s])
            dots[s] = jnp.where(position < lengths_ref[s], scores, -jnp.inf)
        top = {
            s: jnp.maximum(jnp.max(dots[s], axis=-1, keepdims=True), own[s]) for s in members
        }
        weight = {s: jnp.exp(dots[s] - top[s]) for s in members}
        out = {
            s: lax.dot_general(
                weight[s].astype(bf16), values_buf[s], across, preferred_element_type=f32
            )
            for s in members
        }
        for s in members:
            own_weight = jnp.exp(own[s] - top[s])
            total = jnp.sum(weight[s], axis=-1, keepdims=True) + own_weight
            heads_buf[pl.ds(s, heads, stride=rows), :] = (
                out[s] + own_weight * new_value_f[s : s + 1, :]
            ) / total
    new_logsum_ref[...] = turn(eye(rows), collected)
    for h in range(0, heads, 2):
        pair = jnp.concatenate(
            [heads_buf[pl.ds(h * rows, rows), :], heads_buf[pl.ds((h + 1) * rows, rows), :]], axis=1
        )
        for payload_ref in payload_refs:
            payload_ref[:rows, h * HD : (h + 2) * HD] = pair.astype(bf16).astype(payload_ref.dtype)
    outer, half, part = slices_buf.shape
    is_first = lax.axis_index("tp") == 0
    for i in range(outer):
        at = slice(i * part, (i + 1) * part)
        slices_buf[i] = jnp.where(is_first, hidden_buf[:half, at], hidden_buf[half:, at])
    place = lax.axis_index("ep") // (lax.axis_size("ep") // outer)
    for i, payload_ref in enumerate(payload_refs):
        kind = payload_ref.dtype
        payload_ref[rows:, :part] = slices_buf[place ^ i].astype(kind)
        if part < payload_ref.shape[1]:
            payload_ref[rows:, part:] = jnp.zeros((half, payload_ref.shape[1] - part), kind)


def attention(
    hidden, attn_gain, query_weight, key_weight, value_weight, forget_weight, forget_bias,
    cache_keys, cache_values, cache_logsum, lengths, outer,
):
    f32, bf16 = jnp.float32, jnp.bfloat16
    rows, width = hidden.shape
    half = rows // lax.axis_size("tp")
    heads = forget_weight.shape[1]
    cache_len = cache_keys.shape[-1]
    any_spec = pl.BlockSpec(memory_space=pl.ANY)
    args = (
        lengths, hidden, attn_gain, query_weight, key_weight.T, value_weight.T, forget_weight.T,
        forget_bias[None], cache_keys[:, 0], cache_values[:, 0], cache_logsum,
    )
    vmem = pl.BlockSpec(memory_space=pltpu.VMEM)
    bytes_read = sum(a.size * a.dtype.itemsize for a in args)
    *payloads, new_key, new_value, new_logsum = pl.pallas_call(
        attention_kernel,
        out_shape=(
            jax.ShapeDtypeStruct((rows + half, heads * HD), f32),
            *(jax.ShapeDtypeStruct((rows + half, heads * HD), bf16),) * (outer - 1),
            jax.ShapeDtypeStruct((rows, HD), bf16),
            jax.ShapeDtypeStruct((rows, HD), bf16),
            jax.ShapeDtypeStruct((rows, heads), f32),
        ),
        in_specs=[pl.BlockSpec(memory_space=pltpu.SMEM)] + [any_spec] * 10,
        out_specs=(vmem,) * (outer + 3),
        scratch_shapes=[pltpu.VMEM(a.shape, a.dtype) for a in args[1:]]
        + [
            pltpu.VMEM((heads * rows, HD), f32),
            pltpu.VMEM((heads * rows, HD), f32),
            pltpu.VMEM((outer, half, width // outer), bf16),
            pltpu.SemaphoreType.DMA((10 + 3 * GROUPS,)),
        ],
        compiler_params=pltpu.CompilerParams(vmem_limit_bytes=56 * 1024 * 1024),
        cost_estimate=pl.CostEstimate(
            flops=2 * rows * heads * HD * (width + 2 * cache_len),
            bytes_accessed=bytes_read,
            transcendentals=rows * heads * cache_len,
        ),
        name="attention",
    )(*args)
    return payloads, new_key[:, None], new_value[:, None], new_logsum


def project_kernel(outer, inner, *refs):
    f32 = jnp.float32
    payload_refs, refs = refs[:outer], refs[outer:]
    weight_refs, refs = refs[:inner], refs[inner:]
    keep_ref, send_ref, hidden_ref, rows_buf, sums_buf = refs
    rows = rows_buf.shape[0] // outer
    half = payload_refs[0].shape[0] - rows
    part = hidden_ref.shape[1]
    depth = weight_refs[0].shape[0]
    is_first = lax.axis_index("tp") == 0
    index = lax.axis_index("ep")
    place, line = index // inner, index % inner
    for i, payload_ref in enumerate(payload_refs):
        at = place ^ i
        rows_buf[pl.ds(pl.multiple_of(at * rows, rows), rows), :] = payload_ref[:rows, :]
        hidden_ref[pl.ds(pl.multiple_of(at * half, half), half), :] = payload_ref[rows:, :part]
    for i, weight_ref in enumerate(weight_refs):
        sums_buf[line ^ i] = lax.dot_general(
            rows_buf[...], weight_ref[...], (((1,), (1,)), ((), ())), preferred_element_type=f32
        )
    for i in range(inner):
        lanes = slice(i * depth, (i + 1) * depth)
        for k in range(outer):
            low = sums_buf[i, k * rows : k * rows + half, :]
            high = sums_buf[i, k * rows + half : (k + 1) * rows, :]
            at = slice(k * half, (k + 1) * half)
            keep_ref[at, lanes] = jnp.where(is_first, low, high)
            send_ref[at, lanes] = jnp.where(is_first, high, low)


def project(payloads, weights, half):
    f32, bf16 = jnp.float32, jnp.bfloat16
    outer, inner = len(payloads), len(weights)
    rows = payloads[0].shape[0] - half
    depth, width = weights[0].shape
    vmem = pl.BlockSpec(memory_space=pltpu.VMEM)
    total = jax.ShapeDtypeStruct((outer * half, inner * depth), f32)
    return pl.pallas_call(
        functools.partial(project_kernel, outer, inner),
        out_shape=(total, total, jax.ShapeDtypeStruct(total.shape, bf16)),
        in_specs=[vmem] * (outer + inner),
        out_specs=(vmem,) * 3,
        scratch_shapes=[
            pltpu.VMEM((outer * rows, width), bf16),
            pltpu.VMEM((inner, outer * rows, depth), f32),
        ],
        compiler_params=pltpu.CompilerParams(vmem_limit_bytes=VMEM_LIMIT),
        cost_estimate=pl.CostEstimate(
            flops=2 * outer * rows * width * inner * depth,
            bytes_accessed=2 * (outer * rows + inner * depth) * width,
            transcendentals=0,
        ),
        name="project",
    )(*payloads, *weights)


def experts_kernel(outer, inner, blocks_ref, gain_ref, gate_ref, up_ref, *refs):
    f32, bf16 = jnp.float32, jnp.bfloat16
    far_refs, (out_ref, own_ref, inputs_buf, *bufs, sems) = refs[:4], refs[4:]
    _, group, part = blocks_ref.shape
    half = group // outer
    width = outer * part
    fetches = [
        pltpu.make_async_copy(far, buf, sems.at[i])
        for i, (far, buf) in enumerate(zip(far_refs, bufs, strict=True))
    ]
    for fetch in fetches:
        fetch.start()
    gate_other, up_other, down, down_other = bufs
    index = lax.axis_index("ep")
    place, line = index // inner, index % inner
    gain = gain_ref[...].astype(f32).reshape(1, width)
    own_rows = pl.ds(pl.multiple_of(place * half, half), half)
    for z in range(outer):
        lanes = slice(z * part, (z + 1) * part)
        own_ref[:, lanes] = blocks_ref[z * inner + line, own_rows, :]
    for p in range(inner):
        squares = jnp.zeros((group, 1), f32)
        for z in range(outer):
            floats = blocks_ref[z * inner + p].astype(f32)
            squares = squares + jnp.sum(floats * floats, axis=-1, keepdims=True)
        inv_root = lax.rsqrt(squares / width + epsilon)
        for z in range(outer):
            lanes = slice(z * part, (z + 1) * part)
            floats = blocks_ref[z * inner + p].astype(f32)
            inputs_buf[p * group : (p + 1) * group, lanes] = (
                floats * inv_root * gain[:, lanes]
            ).astype(bf16)

    def act(gate_at, up_at):
        gate = jnp.dot(inputs_buf[...], gate_at[...], preferred_element_type=f32)
        up = jnp.dot(inputs_buf[...], up_at[...], preferred_element_type=f32)
        return (gate / (1.0 + jnp.exp(-gate)) * up).astype(bf16)

    for expert in range(gate_ref.shape[0]):
        near_act = act(gate_ref.at[expert], up_ref.at[expert])
        if expert == 0:
            fetches[0].wait()
            fetches[1].wait()
        far_act = act(gate_other.at[expert], up_other.at[expert])
        if expert == 0:
            fetches[2].wait()
            fetches[3].wait()
        total = jnp.dot(near_act, down[expert], preferred_element_type=f32)
        total = total + jnp.dot(far_act, down_other[expert], preferred_element_type=f32)
        for p in range(inner):
            for z in range(outer):
                at = p * group + z * half
                out_ref[z * inner + p, expert] = total[at : at + half].astype(bf16)


def experts(blocks, gain, own, other, outer, inner):
    bf16 = jnp.bfloat16
    ep_size, group, part = blocks.shape
    width = outer * part
    half = group // outer
    rows = ep_size * half
    local, _, depth = own[0].shape
    vmem = pl.BlockSpec(memory_space=pltpu.VMEM)
    outside = pl.BlockSpec(memory_space=pl.ANY)
    far = (other[0], other[1], own[2], other[2])
    return pl.pallas_call(
        functools.partial(experts_kernel, outer, inner),
        out_shape=(
            jax.ShapeDtypeStruct((ep_size, local, half, width), bf16),
            jax.ShapeDtypeStruct((half, width), bf16),
        ),
        in_specs=[vmem] * 4 + [outside] * 4,
        out_specs=(vmem,) * 2,
        scratch_shapes=[
            pltpu.VMEM((rows, width), bf16),
            *(pltpu.VMEM(w.shape, bf16) for w in far),
            pltpu.SemaphoreType.DMA((4,)),
        ],
        compiler_params=pltpu.CompilerParams(vmem_limit_bytes=EXPERTS_LIMIT),
        cost_estimate=pl.CostEstimate(
            flops=12 * local * rows * width * depth,
            bytes_accessed=2 * (2 * rows * width + 6 * local * width * depth),
            transcendentals=2 * local * rows * depth,
        ),
        name="experts",
    )(blocks, gain, own[0], own[1], *far)


def combine_kernel(returned_ref, ids_ref, scores_ref, own_ref, out_ref):
    f32 = jnp.float32
    ep_size, local, half, width = returned_ref.shape
    top, rows = ids_ref.shape
    square = (rows, rows)
    same = lax.broadcasted_iota(jnp.int32, square, 0) == lax.broadcasted_iota(jnp.int32, square, 1)
    turn = functools.partial(
        lax.dot_general,
        same.astype(f32),
        dimension_numbers=(((1,), (1,)), ((), ())),
        preferred_element_type=f32,
        precision=lax.Precision.HIGHEST,
    )
    scores = scores_ref[...]
    ids = turn(ids_ref[...].astype(f32))
    route = turn(scores / jnp.sum(scores, axis=0, keepdims=True))
    is_first = lax.axis_index("tp") == 0
    ids = jnp.where(is_first, ids[:half], ids[half:])
    route = jnp.where(is_first, route[:half], route[half:])
    expert = lax.broadcasted_iota(jnp.int32, (half, ep_size * local), 1).astype(f32)
    weight = jnp.zeros((half, ep_size * local), f32)
    for k in range(top):
        weight = weight + jnp.where(ids[:, k : k + 1] == expert, route[:, k : k + 1], 0.0)
    total = own_ref[...].astype(f32)
    mix = jnp.zeros((half, width), f32)
    for e in range(ep_size):
        for i in range(local):
            at = e * local + i
            mix = mix + returned_ref[e, i].astype(f32) * weight[:, at : at + 1]
    out_ref[...] = (total + mix).astype(out_ref.dtype)


def combine(returned, ids, scores, own):
    vmem = pl.BlockSpec(memory_space=pltpu.VMEM)
    return pl.pallas_call(
        combine_kernel,
        out_shape=jax.ShapeDtypeStruct(own.shape, own.dtype),
        in_specs=[vmem] * 4,
        out_specs=vmem,
        compiler_params=pltpu.CompilerParams(vmem_limit_bytes=VMEM_LIMIT),
        cost_estimate=pl.CostEstimate(
            flops=2 * returned.size, bytes_accessed=2 * returned.size, transcendentals=0
        ),
        name="combine",
    )(returned, ids.T, scores.T, own)


def over_lines(arrays, inner):
    ep_size, outer = lax.axis_size("ep"), len(arrays)
    if outer <= 4:
        return arrays[:1] + [
            lax.ppermute(a, "ep", [(e, e ^ (i * inner)) for e in range(ep_size)])
            for i, a in list(enumerate(arrays))[1:]
        ]
    place = lax.axis_index("ep") // inner
    order = jnp.arange(outer, dtype=jnp.int32) ^ place
    groups = [[z * inner + p for z in range(outer)] for p in range(inner)]
    moved = lax.all_to_all(
        jnp.stack(arrays)[order], "ep", 0, 0, axis_index_groups=groups, tiled=True
    )
    return list(moved[order])


def per_device(
    hidden,
    attn_gain,
    query_weight,
    key_weight,
    value_weight,
    forget_weight,
    forget_bias,
    cache_keys,
    cache_values,
    cache_logsum,
    lengths,
    out_weight,
    ffn_gain,
    expert_ids,
    expert_scores,
    gate_weights,
    up_weights,
    down_weights,
):
    f32, bf16 = jnp.float32, jnp.bfloat16
    rows_here, width = hidden.shape
    ep_size, tp_size = lax.axis_size("ep"), lax.axis_size("tp")
    tp_index = lax.axis_index("tp")
    is_first = tp_index == 0
    half = rows_here // tp_size
    local_experts = gate_weights.shape[0]

    gate_other = lax.ppermute(gate_weights, "tp", SWAP)
    up_other = lax.ppermute(up_weights, "tp", SWAP)
    down_other = lax.ppermute(down_weights, "tp", SWAP)

    inner = 4 if ep_size % 4 == 0 else 1
    outer = ep_size // inner
    heads_here = query_weight.shape[1]
    with jax.named_scope("share"):
        weight_half = lax.dynamic_slice_in_dim(out_weight, tp_index * heads_here, heads_here, 1)
        shared = [weight_half] + [
            lax.ppermute(weight_half, "ep", [(e, e ^ i) for e in range(ep_size)])
            for i in range(1, inner)
        ]
    with jax.named_scope("attend"):
        payloads, key_new, value_new, new_logsum = attention(
            hidden,
            attn_gain,
            query_weight,
            key_weight,
            value_weight,
            forget_weight,
            forget_bias,
            cache_keys,
            cache_values,
            cache_logsum,
            lengths,
            outer,
        )
    payloads[0] = payloads[0].astype(bf16)
    with jax.named_scope("lines"):
        payloads = over_lines(payloads, inner)
    keep, send, hidden_part = project(payloads, shared, half)
    mixed = (keep + lax.ppermute(send, "tp", SWAP)).astype(bf16)
    residual_part = (hidden_part.astype(f32) + mixed.astype(f32)).astype(bf16)

    blocks = lax.all_to_all(
        jnp.broadcast_to(residual_part[None], (ep_size,) + residual_part.shape),
        "ep",
        split_axis=0,
        concat_axis=0,
        tiled=True,
    )
    outgoing, own = experts(
        blocks,
        ffn_gain,
        (gate_weights, up_weights, down_weights),
        (gate_other, up_other, down_other),
        outer,
        inner,
    )
    returned = lax.all_to_all(outgoing, "ep", split_axis=0, concat_axis=0, tiled=True)

    updated_mine = combine(returned, expert_ids, expert_scores, own)
    updated_theirs = lax.ppermute(updated_mine, "tp", SWAP)
    updated = jnp.concatenate(
        [
            jnp.where(is_first, updated_mine, updated_theirs),
            jnp.where(is_first, updated_theirs, updated_mine),
        ],
        axis=0,
    )
    return (updated, key_new, value_new, new_logsum)
def solution(mesh):
    in_specs = (
        P("ep", None),
        P(),
        P(None, "tp"),
        P(None, "tp"),
        P(None, "tp"),
        P(None, "tp"),
        P("tp"),
        P("ep", "tp", None, None),
        P("ep", "tp", None, None),
        P("ep", "tp", None),
        P("ep"),
        P("ep", None),
        P(),
        P("ep", None),
        P("ep", None),
        P("ep", None, "tp"),
        P("ep", None, "tp"),
        P("ep", "tp", None),
    )
    out_specs = (P("ep", None), P("ep", "tp", None), P("ep", "tp", None), P("ep", "tp"))
    return jax.shard_map(
        per_device, mesh=mesh, in_specs=in_specs, out_specs=out_specs, check_vma=False
    )
```

```python
import functools

import jax
import jax.numpy as jnp
from jax import lax
from jax.experimental import pallas as pl
from jax.experimental.pallas import tpu as pltpu
from jax.sharding import PartitionSpec as P

HD = 64
GROUPS = 2
EXPERTS_LIMIT = 16 * 1024 * 1024
VMEM_LIMIT = 24 * 1024 * 1024

epsilon = 1e-06
SWAP = ((0, 1), (1, 0))


def attention_kernel(
    lengths_ref, hidden_ref, gain_ref, query_ref, key_ref, value_ref, forget_ref, bias_ref,
    keys_ref, values_ref, logsum_ref,
    *refs,
):
    (
        *payload_refs, new_key_ref, new_value_ref, new_logsum_ref,
        hidden_buf, gain_buf, query_buf, key_buf, value_buf, forget_buf, bias_buf,
        keys_buf, values_buf, logsum_buf, queries_buf, heads_buf, slices_buf, sems,
    ) = refs
    f32, bf16 = jnp.float32, jnp.bfloat16
    rows, width = hidden_buf.shape
    heads = forget_buf.shape[0]
    cache_len = keys_buf.shape[-1]
    count = [0]

    def fetch(source, target):
        copy = pltpu.make_async_copy(source, target, sems.at[count[0]])
        count[0] += 1
        copy.start()
        return copy

    small = [
        fetch(a, b)
        for a, b in (
            (hidden_ref, hidden_buf),
            (gain_ref, gain_buf),
            (bias_ref, bias_buf),
            (forget_ref, forget_buf),
            (key_ref, key_buf),
            (value_ref, value_buf),
        )
    ]
    parts = 4
    depth = width // parts
    query_copies = [
        fetch(query_ref.at[pl.ds(i * depth, depth)], query_buf.at[pl.ds(i * depth, depth)])
        for i in range(parts)
    ]
    group = rows // GROUPS
    past = []
    for i in range(GROUPS):
        at = pl.ds(i * group, group)
        past.append(
            [
                fetch(a.at[at], b.at[at])
                for a, b in (
                    (logsum_ref, logsum_buf), (keys_ref, keys_buf), (values_ref, values_buf)
                )
            ]
        )

    for copy in small:
        copy.wait()
    floats = hidden_buf[...].astype(f32)
    inv_root = lax.rsqrt(jnp.mean(floats * floats, axis=-1, keepdims=True) + epsilon)
    normed = (floats * inv_root * gain_buf[...].astype(f32).reshape(1, width)).astype(bf16)
    across = (((1,), (1,)), ((), ()))
    new_key = lax.dot_general(normed, key_buf[...], across, preferred_element_type=f32).astype(bf16)
    new_value = lax.dot_general(normed, value_buf[...], across, preferred_element_type=f32).astype(bf16)
    new_key_ref[...] = new_key
    new_value_ref[...] = new_value
    logits = lax.dot_general(normed, forget_buf[...], across, preferred_element_type=f32) + bias_buf[...]
    log_forget = jnp.minimum(logits, 0.0) - jnp.log1p(jnp.exp(-jnp.abs(logits)))
    turn = functools.partial(
        lax.dot_general, dimension_numbers=across, preferred_element_type=f32,
        precision=lax.Precision.HIGHEST,
    )

    def eye(size):
        return (
            lax.broadcasted_iota(jnp.int32, (size, size), 0)
            == lax.broadcasted_iota(jnp.int32, (size, size), 1)
        ).astype(f32)

    log_forget = turn(eye(heads), log_forget)
    queries = jnp.zeros((rows, heads * HD), f32)
    for i, copy in enumerate(query_copies):
        copy.wait()
        at = slice(i * depth, (i + 1) * depth)
        queries = queries + jnp.dot(normed[:, at], query_buf[at, :], preferred_element_type=f32)
    queries = queries.astype(bf16).astype(f32) * HD ** (-0.5)
    for h in range(heads):
        queries_buf[pl.ds(h * rows, rows), :] = queries[:, h * HD : (h + 1) * HD]
    new_key_f, new_value_f = new_key.astype(f32), new_value.astype(f32)
    lane = lax.broadcasted_iota(jnp.int32, (heads, 128), 1)
    position = lax.broadcasted_iota(jnp.int32, (heads, cache_len), 1)
    column = lax.broadcasted_iota(jnp.int32, (heads, rows), 1)
    collected = jnp.zeros((heads, rows), f32)
    for first in range(0, rows, group):
        for copy in past[first // group]:
            copy.wait()
        members = range(first, first + group)
        query = {s: queries_buf[pl.ds(s, heads, stride=rows), :] for s in members}
        dots = {
            s: jnp.dot(query[s].astype(bf16), keys_buf[s], preferred_element_type=f32)
            for s in members
        }
        newest, own = {}, {}
        for s in members:
            last_at = lengths_ref[s] - 1
            base = pl.multiple_of(last_at // 128 * 128, 128)
            last = logsum_buf[s, :, pl.ds(base, 128)]
            last = jnp.where(lane == last_at - base, last, 0.0)
            newest[s] = jnp.sum(last, axis=-1, keepdims=True) + log_forget[:, s : s + 1]
            own[s] = jnp.sum(query[s] * new_key_f[s : s + 1, :], axis=-1, keepdims=True)
        for s in members:
            collected = jnp.where(column == s, newest[s], collected)
            scores = dots[s] + (newest[s] - logsum_buf[s])
            dots[s] = jnp.where(position < lengths_ref[s], scores, -jnp.inf)
        top = {
            s: jnp.maximum(jnp.max(dots[s], axis=-1, keepdims=True), own[s]) for s in members
        }
        weight = {s: jnp.exp(dots[s] - top[s]) for s in members}
        out = {
            s: lax.dot_general(
                weight[s].astype(bf16), values_buf[s], across, preferred_element_type=f32
            )
            for s in members
        }
        for s in members:
            own_weight = jnp.exp(own[s] - top[s])
            total = jnp.sum(weight[s], axis=-1, keepdims=True) + own_weight
            heads_buf[pl.ds(s, heads, stride=rows), :] = (
                out[s] + own_weight * new_value_f[s : s + 1, :]
            ) / total
    new_logsum_ref[...] = turn(eye(rows), collected)
    for h in range(0, heads, 2):
        pair = jnp.concatenate(
            [heads_buf[pl.ds(h * rows, rows), :], heads_buf[pl.ds((h + 1) * rows, rows), :]], axis=1
        )
        for payload_ref in payload_refs:
            payload_ref[:rows, h * HD : (h + 2) * HD] = pair.astype(bf16).astype(payload_ref.dtype)
    outer, half, part = slices_buf.shape
    is_first = lax.axis_index("tp") == 0
    for i in range(outer):
        at = slice(i * part, (i + 1) * part)
        slices_buf[i] = jnp.where(is_first, hidden_buf[:half, at], hidden_buf[half:, at])
    place = lax.axis_index("ep") // (lax.axis_size("ep") // outer)
    for i, payload_ref in enumerate(payload_refs):
        kind = payload_ref.dtype
        payload_ref[rows:, :part] = slices_buf[place ^ i].astype(kind)
        if part < payload_ref.shape[1]:
            payload_ref[rows:, part:] = jnp.zeros((half, payload_ref.shape[1] - part), kind)


def attention(
    hidden, attn_gain, query_weight, key_weight, value_weight, forget_weight, forget_bias,
    cache_keys, cache_values, cache_logsum, lengths, outer,
):
    f32, bf16 = jnp.float32, jnp.bfloat16
    rows, width = hidden.shape
    half = rows // lax.axis_size("tp")
    heads = forget_weight.shape[1]
    cache_len = cache_keys.shape[-1]
    any_spec = pl.BlockSpec(memory_space=pl.ANY)
    args = (
        lengths, hidden, attn_gain, query_weight, key_weight.T, value_weight.T, forget_weight.T,
        forget_bias[None], cache_keys[:, 0], cache_values[:, 0], cache_logsum,
    )
    vmem = pl.BlockSpec(memory_space=pltpu.VMEM)
    bytes_read = sum(a.size * a.dtype.itemsize for a in args)
    *payloads, new_key, new_value, new_logsum = pl.pallas_call(
        attention_kernel,
        out_shape=(
            jax.ShapeDtypeStruct((rows + half, heads * HD), f32),
            *(jax.ShapeDtypeStruct((rows + half, heads * HD), bf16),) * (outer - 1),
            jax.ShapeDtypeStruct((rows, HD), bf16),
            jax.ShapeDtypeStruct((rows, HD), bf16),
            jax.ShapeDtypeStruct((rows, heads), f32),
        ),
        in_specs=[pl.BlockSpec(memory_space=pltpu.SMEM)] + [any_spec] * 10,
        out_specs=(vmem,) * (outer + 3),
        scratch_shapes=[pltpu.VMEM(a.shape, a.dtype) for a in args[1:]]
        + [
            pltpu.VMEM((heads * rows, HD), f32),
            pltpu.VMEM((heads * rows, HD), f32),
            pltpu.VMEM((outer, half, width // outer), bf16),
            pltpu.SemaphoreType.DMA((10 + 3 * GROUPS,)),
        ],
        compiler_params=pltpu.CompilerParams(vmem_limit_bytes=56 * 1024 * 1024),
        cost_estimate=pl.CostEstimate(
            flops=2 * rows * heads * HD * (width + 2 * cache_len),
            bytes_accessed=bytes_read,
            transcendentals=rows * heads * cache_len,
        ),
        name="attention",
    )(*args)
    return payloads, new_key[:, None], new_value[:, None], new_logsum


def project_kernel(outer, inner, *refs):
    f32 = jnp.float32
    payload_refs, refs = refs[:outer], refs[outer:]
    weight_refs, refs = refs[:inner], refs[inner:]
    keep_ref, send_ref, hidden_ref, rows_buf, sums_buf = refs
    rows = rows_buf.shape[0] // outer
    half = payload_refs[0].shape[0] - rows
    part = hidden_ref.shape[1]
    depth = weight_refs[0].shape[0]
    is_first = lax.axis_index("tp") == 0
    index = lax.axis_index("ep")
    place, line = index // inner, index % inner
    for i, payload_ref in enumerate(payload_refs):
        at = place ^ i
        rows_buf[pl.ds(pl.multiple_of(at * rows, rows), rows), :] = payload_ref[:rows, :]
        hidden_ref[pl.ds(pl.multiple_of(at * half, half), half), :] = payload_ref[rows:, :part]
    for i, weight_ref in enumerate(weight_refs):
        sums_buf[line ^ i] = lax.dot_general(
            rows_buf[...], weight_ref[...], (((1,), (1,)), ((), ())), preferred_element_type=f32
        )
    for i in range(inner):
        lanes = slice(i * depth, (i + 1) * depth)
        for k in range(outer):
            low = sums_buf[i, k * rows : k * rows + half, :]
            high = sums_buf[i, k * rows + half : (k + 1) * rows, :]
            at = slice(k * half, (k + 1) * half)
            keep_ref[at, lanes] = jnp.where(is_first, low, high)
            send_ref[at, lanes] = jnp.where(is_first, high, low)


def project(payloads, weights, half):
    f32, bf16 = jnp.float32, jnp.bfloat16
    outer, inner = len(payloads), len(weights)
    rows = payloads[0].shape[0] - half
    depth, width = weights[0].shape
    vmem = pl.BlockSpec(memory_space=pltpu.VMEM)
    total = jax.ShapeDtypeStruct((outer * half, inner * depth), f32)
    return pl.pallas_call(
        functools.partial(project_kernel, outer, inner),
        out_shape=(total, total, jax.ShapeDtypeStruct(total.shape, bf16)),
        in_specs=[vmem] * (outer + inner),
        out_specs=(vmem,) * 3,
        scratch_shapes=[
            pltpu.VMEM((outer * rows, width), bf16),
            pltpu.VMEM((inner, outer * rows, depth), f32),
        ],
        compiler_params=pltpu.CompilerParams(vmem_limit_bytes=VMEM_LIMIT),
        cost_estimate=pl.CostEstimate(
            flops=2 * outer * rows * width * inner * depth,
            bytes_accessed=2 * (outer * rows + inner * depth) * width,
            transcendentals=0,
        ),
        name="project",
    )(*payloads, *weights)


def experts_kernel(outer, inner, blocks_ref, gain_ref, gate_ref, up_ref, down_ref, *refs):
    f32, bf16 = jnp.float32, jnp.bfloat16
    far_refs, (out_ref, own_ref, inputs_buf, sums_buf, *bufs, sems) = refs[:3], refs[3:]
    _, group, part = blocks_ref.shape
    half = group // outer
    width = outer * part
    fetches = [
        pltpu.make_async_copy(far, buf, sems.at[i])
        for i, (far, buf) in enumerate(zip(far_refs, bufs, strict=True))
    ]
    for fetch in fetches:
        fetch.start()
    gate_other, up_other, down_other = bufs
    index = lax.axis_index("ep")
    place, line = index // inner, index % inner
    gain = gain_ref[...].astype(f32).reshape(1, width)
    own_rows = pl.ds(pl.multiple_of(place * half, half), half)
    for z in range(outer):
        lanes = slice(z * part, (z + 1) * part)
        own_ref[:, lanes] = blocks_ref[z * inner + line, own_rows, :]
    for p in range(inner):
        squares = jnp.zeros((group, 1), f32)
        for z in range(outer):
            floats = blocks_ref[z * inner + p].astype(f32)
            squares = squares + jnp.sum(floats * floats, axis=-1, keepdims=True)
        inv_root = lax.rsqrt(squares / width + epsilon)
        for z in range(outer):
            lanes = slice(z * part, (z + 1) * part)
            floats = blocks_ref[z * inner + p].astype(f32)
            inputs_buf[p * group : (p + 1) * group, lanes] = (
                floats * inv_root * gain[:, lanes]
            ).astype(bf16)

    def act(gate_at, up_at):
        gate = jnp.dot(inputs_buf[...], gate_at[...], preferred_element_type=f32)
        up = jnp.dot(inputs_buf[...], up_at[...], preferred_element_type=f32)
        return (gate / (1.0 + jnp.exp(-gate)) * up).astype(bf16)

    for expert in range(gate_ref.shape[0]):
        near_act = act(gate_ref.at[expert], up_ref.at[expert])
        sums_buf[...] = jnp.dot(near_act, down_ref[expert], preferred_element_type=f32)
        if expert == 0:
            fetches[0].wait()
            fetches[1].wait()
        far_act = act(gate_other.at[expert], up_other.at[expert])
        if expert == 0:
            fetches[2].wait()
        total = sums_buf[...] + jnp.dot(
            far_act, down_other[expert], preferred_element_type=f32
        )
        for p in range(inner):
            for z in range(outer):
                at = p * group + z * half
                out_ref[z * inner + p, expert] = total[at : at + half].astype(bf16)


def experts(blocks, gain, own, other, outer, inner):
    bf16 = jnp.bfloat16
    ep_size, group, part = blocks.shape
    width = outer * part
    half = group // outer
    rows = ep_size * half
    local, _, depth = own[0].shape
    vmem = pl.BlockSpec(memory_space=pltpu.VMEM)
    outside = pl.BlockSpec(memory_space=pl.ANY)
    return pl.pallas_call(
        functools.partial(experts_kernel, outer, inner),
        out_shape=(
            jax.ShapeDtypeStruct((ep_size, local, half, width), bf16),
            jax.ShapeDtypeStruct((half, width), bf16),
        ),
        in_specs=[vmem] * 5 + [outside] * 3,
        out_specs=(vmem,) * 2,
        scratch_shapes=[
            pltpu.VMEM((rows, width), bf16),
            pltpu.VMEM((rows, width), jnp.float32),
            *(pltpu.VMEM(w.shape, bf16) for w in other),
            pltpu.SemaphoreType.DMA((3,)),
        ],
        compiler_params=pltpu.CompilerParams(vmem_limit_bytes=EXPERTS_LIMIT),
        cost_estimate=pl.CostEstimate(
            flops=12 * local * rows * width * depth,
            bytes_accessed=2 * (2 * rows * width + 6 * local * width * depth),
            transcendentals=2 * local * rows * depth,
        ),
        name="experts",
    )(blocks, gain, *own, *other)


def combine_kernel(returned_ref, ids_ref, scores_ref, own_ref, out_ref):
    f32 = jnp.float32
    ep_size, local, half, width = returned_ref.shape
    top, rows = ids_ref.shape
    square = (rows, rows)
    same = lax.broadcasted_iota(jnp.int32, square, 0) == lax.broadcasted_iota(jnp.int32, square, 1)
    turn = functools.partial(
        lax.dot_general,
        same.astype(f32),
        dimension_numbers=(((1,), (1,)), ((), ())),
        preferred_element_type=f32,
        precision=lax.Precision.HIGHEST,
    )
    scores = scores_ref[...]
    ids = turn(ids_ref[...].astype(f32))
    route = turn(scores / jnp.sum(scores, axis=0, keepdims=True))
    is_first = lax.axis_index("tp") == 0
    ids = jnp.where(is_first, ids[:half], ids[half:])
    route = jnp.where(is_first, route[:half], route[half:])
    expert = lax.broadcasted_iota(jnp.int32, (half, ep_size * local), 1).astype(f32)
    weight = jnp.zeros((half, ep_size * local), f32)
    for k in range(top):
        weight = weight + jnp.where(ids[:, k : k + 1] == expert, route[:, k : k + 1], 0.0)
    total = own_ref[...].astype(f32)
    mix = jnp.zeros((half, width), f32)
    for e in range(ep_size):
        for i in range(local):
            at = e * local + i
            mix = mix + returned_ref[e, i].astype(f32) * weight[:, at : at + 1]
    out_ref[...] = (total + mix).astype(out_ref.dtype)


def combine(returned, ids, scores, own):
    vmem = pl.BlockSpec(memory_space=pltpu.VMEM)
    return pl.pallas_call(
        combine_kernel,
        out_shape=jax.ShapeDtypeStruct(own.shape, own.dtype),
        in_specs=[vmem] * 4,
        out_specs=vmem,
        compiler_params=pltpu.CompilerParams(vmem_limit_bytes=VMEM_LIMIT),
        cost_estimate=pl.CostEstimate(
            flops=2 * returned.size, bytes_accessed=2 * returned.size, transcendentals=0
        ),
        name="combine",
    )(returned, ids.T, scores.T, own)


def over_lines(arrays, inner):
    ep_size, outer = lax.axis_size("ep"), len(arrays)
    if outer <= 4:
        return arrays[:1] + [
            lax.ppermute(a, "ep", [(e, e ^ (i * inner)) for e in range(ep_size)])
            for i, a in list(enumerate(arrays))[1:]
        ]
    place = lax.axis_index("ep") // inner
    order = jnp.arange(outer, dtype=jnp.int32) ^ place
    groups = [[z * inner + p for z in range(outer)] for p in range(inner)]
    moved = lax.all_to_all(
        jnp.stack(arrays)[order], "ep", 0, 0, axis_index_groups=groups, tiled=True
    )
    return list(moved[order])


def per_device(
    hidden,
    attn_gain,
    query_weight,
    key_weight,
    value_weight,
    forget_weight,
    forget_bias,
    cache_keys,
    cache_values,
    cache_logsum,
    lengths,
    out_weight,
    ffn_gain,
    expert_ids,
    expert_scores,
    gate_weights,
    up_weights,
    down_weights,
):
    f32, bf16 = jnp.float32, jnp.bfloat16
    rows_here, width = hidden.shape
    ep_size, tp_size = lax.axis_size("ep"), lax.axis_size("tp")
    tp_index = lax.axis_index("tp")
    is_first = tp_index == 0
    half = rows_here // tp_size
    local_experts = gate_weights.shape[0]

    gate_other = lax.ppermute(gate_weights, "tp", SWAP)
    up_other = lax.ppermute(up_weights, "tp", SWAP)
    down_other = lax.ppermute(down_weights, "tp", SWAP)

    inner = 4 if ep_size % 4 == 0 else 1
    outer = ep_size // inner
    heads_here = query_weight.shape[1]
    with jax.named_scope("share"):
        weight_half = lax.dynamic_slice_in_dim(out_weight, tp_index * heads_here, heads_here, 1)
        shared = [weight_half] + [
            lax.ppermute(weight_half, "ep", [(e, e ^ i) for e in range(ep_size)])
            for i in range(1, inner)
        ]
    with jax.named_scope("attend"):
        payloads, key_new, value_new, new_logsum = attention(
            hidden,
            attn_gain,
            query_weight,
            key_weight,
            value_weight,
            forget_weight,
            forget_bias,
            cache_keys,
            cache_values,
            cache_logsum,
            lengths,
            outer,
        )
    payloads[0] = payloads[0].astype(bf16)
    with jax.named_scope("lines"):
        payloads = over_lines(payloads, inner)
    keep, send, hidden_part = project(payloads, shared, half)
    mixed = (keep + lax.ppermute(send, "tp", SWAP)).astype(bf16)
    residual_part = (hidden_part.astype(f32) + mixed.astype(f32)).astype(bf16)

    residual_part, gate_other, up_other, down_other = lax.optimization_barrier(
        (residual_part, gate_other, up_other, down_other)
    )
    blocks = lax.all_to_all(
        jnp.broadcast_to(residual_part[None], (ep_size,) + residual_part.shape),
        "ep",
        split_axis=0,
        concat_axis=0,
        tiled=True,
    )
    outgoing, own = experts(
        blocks,
        ffn_gain,
        (gate_weights, up_weights, down_weights),
        (gate_other, up_other, down_other),
        outer,
        inner,
    )
    returned = lax.all_to_all(outgoing, "ep", split_axis=0, concat_axis=0, tiled=True)

    updated_mine = combine(returned, expert_ids, expert_scores, own)
    updated_theirs = lax.ppermute(updated_mine, "tp", SWAP)
    updated = jnp.concatenate(
        [
            jnp.where(is_first, updated_mine, updated_theirs),
            jnp.where(is_first, updated_theirs, updated_mine),
        ],
        axis=0,
    )
    return (updated, key_new, value_new, new_logsum)
def solution(mesh):
    in_specs = (
        P("ep", None),
        P(),
        P(None, "tp"),
        P(None, "tp"),
        P(None, "tp"),
        P(None, "tp"),
        P("tp"),
        P("ep", "tp", None, None),
        P("ep", "tp", None, None),
        P("ep", "tp", None),
        P("ep"),
        P("ep", None),
        P(),
        P("ep", None),
        P("ep", None),
        P("ep", None, "tp"),
        P("ep", None, "tp"),
        P("ep", "tp", None),
    )
    out_specs = (P("ep", None), P("ep", "tp", None), P("ep", "tp", None), P("ep", "tp"))
    return jax.shard_map(
        per_device, mesh=mesh, in_specs=in_specs, out_specs=out_specs, check_vma=False
    )
```

```python
import functools

import jax
import jax.numpy as jnp
from jax import lax
from jax.experimental import pallas as pl
from jax.experimental.pallas import tpu as pltpu
from jax.sharding import PartitionSpec as P

HD = 64
GROUPS = 2
EXPERTS_LIMIT = 16 * 1024 * 1024
VMEM_LIMIT = 24 * 1024 * 1024

epsilon = 1e-06
SWAP = ((0, 1), (1, 0))


def attention_kernel(
    lengths_ref, hidden_ref, gain_ref, query_ref, key_ref, value_ref, forget_ref, bias_ref,
    keys_ref, values_ref, logsum_ref,
    *refs,
):
    (
        *payload_refs, new_key_ref, new_value_ref, new_logsum_ref,
        hidden_buf, gain_buf, query_buf, key_buf, value_buf, forget_buf, bias_buf,
        keys_buf, values_buf, logsum_buf, queries_buf, heads_buf, slices_buf, sems,
    ) = refs
    f32, bf16 = jnp.float32, jnp.bfloat16
    rows, width = hidden_buf.shape
    heads = forget_buf.shape[0]
    cache_len = keys_buf.shape[-1]
    count = [0]

    def fetch(source, target):
        copy = pltpu.make_async_copy(source, target, sems.at[count[0]])
        count[0] += 1
        copy.start()
        return copy

    small = [
        fetch(a, b)
        for a, b in (
            (hidden_ref, hidden_buf),
            (gain_ref, gain_buf),
            (bias_ref, bias_buf),
            (forget_ref, forget_buf),
            (key_ref, key_buf),
            (value_ref, value_buf),
        )
    ]
    parts = 4
    depth = width // parts
    query_copies = [
        fetch(query_ref.at[pl.ds(i * depth, depth)], query_buf.at[pl.ds(i * depth, depth)])
        for i in range(parts)
    ]
    group = rows // GROUPS
    past = []
    for i in range(GROUPS):
        at = pl.ds(i * group, group)
        past.append(
            [
                fetch(a.at[at], b.at[at])
                for a, b in (
                    (logsum_ref, logsum_buf), (keys_ref, keys_buf), (values_ref, values_buf)
                )
            ]
        )

    for copy in small:
        copy.wait()
    floats = hidden_buf[...].astype(f32)
    inv_root = lax.rsqrt(jnp.mean(floats * floats, axis=-1, keepdims=True) + epsilon)
    normed = (floats * inv_root * gain_buf[...].astype(f32).reshape(1, width)).astype(bf16)
    across = (((1,), (1,)), ((), ()))
    new_key = lax.dot_general(normed, key_buf[...], across, preferred_element_type=f32).astype(bf16)
    new_value = lax.dot_general(normed, value_buf[...], across, preferred_element_type=f32).astype(bf16)
    new_key_ref[...] = new_key
    new_value_ref[...] = new_value
    logits = lax.dot_general(normed, forget_buf[...], across, preferred_element_type=f32) + bias_buf[...]
    log_forget = jnp.minimum(logits, 0.0) - jnp.log1p(jnp.exp(-jnp.abs(logits)))
    turn = functools.partial(
        lax.dot_general, dimension_numbers=across, preferred_element_type=f32,
        precision=lax.Precision.HIGHEST,
    )

    def eye(size):
        return (
            lax.broadcasted_iota(jnp.int32, (size, size), 0)
            == lax.broadcasted_iota(jnp.int32, (size, size), 1)
        ).astype(f32)

    log_forget = turn(eye(heads), log_forget)
    queries = jnp.zeros((rows, heads * HD), f32)
    for i, copy in enumerate(query_copies):
        copy.wait()
        at = slice(i * depth, (i + 1) * depth)
        queries = queries + jnp.dot(normed[:, at], query_buf[at, :], preferred_element_type=f32)
    queries = queries.astype(bf16).astype(f32) * HD ** (-0.5)
    for h in range(heads):
        queries_buf[pl.ds(h * rows, rows), :] = queries[:, h * HD : (h + 1) * HD]
    new_key_f, new_value_f = new_key.astype(f32), new_value.astype(f32)
    lane = lax.broadcasted_iota(jnp.int32, (heads, 128), 1)
    position = lax.broadcasted_iota(jnp.int32, (heads, cache_len), 1)
    column = lax.broadcasted_iota(jnp.int32, (heads, rows), 1)
    collected = jnp.zeros((heads, rows), f32)
    for first in range(0, rows, group):
        *needed, values_copy = past[first // group]
        for copy in needed:
            copy.wait()
        members = range(first, first + group)
        query = {s: queries_buf[pl.ds(s, heads, stride=rows), :] for s in members}
        dots = {
            s: jnp.dot(query[s].astype(bf16), keys_buf[s], preferred_element_type=f32)
            for s in members
        }
        newest, own = {}, {}
        for s in members:
            last_at = lengths_ref[s] - 1
            base = pl.multiple_of(last_at // 128 * 128, 128)
            last = logsum_buf[s, :, pl.ds(base, 128)]
            last = jnp.where(lane == last_at - base, last, 0.0)
            newest[s] = jnp.sum(last, axis=-1, keepdims=True) + log_forget[:, s : s + 1]
            own[s] = jnp.sum(query[s] * new_key_f[s : s + 1, :], axis=-1, keepdims=True)
        for s in members:
            collected = jnp.where(column == s, newest[s], collected)
            scores = dots[s] + (newest[s] - logsum_buf[s])
            dots[s] = jnp.where(position < lengths_ref[s], scores, -jnp.inf)
        top = {
            s: jnp.maximum(jnp.max(dots[s], axis=-1, keepdims=True), own[s]) for s in members
        }
        weight = {s: jnp.exp(dots[s] - top[s]) for s in members}
        values_copy.wait()
        out = {
            s: lax.dot_general(
                weight[s].astype(bf16), values_buf[s], across, preferred_element_type=f32
            )
            for s in members
        }
        for s in members:
            own_weight = jnp.exp(own[s] - top[s])
            total = jnp.sum(weight[s], axis=-1, keepdims=True) + own_weight
            heads_buf[pl.ds(s, heads, stride=rows), :] = (
                out[s] + own_weight * new_value_f[s : s + 1, :]
            ) / total
    new_logsum_ref[...] = turn(eye(rows), collected)
    for h in range(0, heads, 2):
        pair = jnp.concatenate(
            [heads_buf[pl.ds(h * rows, rows), :], heads_buf[pl.ds((h + 1) * rows, rows), :]], axis=1
        )
        for payload_ref in payload_refs:
            payload_ref[:rows, h * HD : (h + 2) * HD] = pair.astype(bf16).astype(payload_ref.dtype)
    outer, half, part = slices_buf.shape
    is_first = lax.axis_index("tp") == 0
    for i in range(outer):
        at = slice(i * part, (i + 1) * part)
        slices_buf[i] = jnp.where(is_first, hidden_buf[:half, at], hidden_buf[half:, at])
    place = lax.axis_index("ep") // (lax.axis_size("ep") // outer)
    for i, payload_ref in enumerate(payload_refs):
        kind = payload_ref.dtype
        payload_ref[rows:, :part] = slices_buf[place ^ i].astype(kind)
        if part < payload_ref.shape[1]:
            payload_ref[rows:, part:] = jnp.zeros((half, payload_ref.shape[1] - part), kind)


def attention(
    hidden, attn_gain, query_weight, key_weight, value_weight, forget_weight, forget_bias,
    cache_keys, cache_values, cache_logsum, lengths, outer,
):
    f32, bf16 = jnp.float32, jnp.bfloat16
    rows, width = hidden.shape
    half = rows // lax.axis_size("tp")
    heads = forget_weight.shape[1]
    cache_len = cache_keys.shape[-1]
    any_spec = pl.BlockSpec(memory_space=pl.ANY)
    args = (
        lengths, hidden, attn_gain, query_weight, key_weight.T, value_weight.T, forget_weight.T,
        forget_bias[None], cache_keys[:, 0], cache_values[:, 0], cache_logsum,
    )
    vmem = pl.BlockSpec(memory_space=pltpu.VMEM)
    bytes_read = sum(a.size * a.dtype.itemsize for a in args)
    *payloads, new_key, new_value, new_logsum = pl.pallas_call(
        attention_kernel,
        out_shape=(
            jax.ShapeDtypeStruct((rows + half, heads * HD), f32),
            *(jax.ShapeDtypeStruct((rows + half, heads * HD), bf16),) * (outer - 1),
            jax.ShapeDtypeStruct((rows, HD), bf16),
            jax.ShapeDtypeStruct((rows, HD), bf16),
            jax.ShapeDtypeStruct((rows, heads), f32),
        ),
        in_specs=[pl.BlockSpec(memory_space=pltpu.SMEM)] + [any_spec] * 10,
        out_specs=(vmem,) * (outer + 3),
        scratch_shapes=[pltpu.VMEM(a.shape, a.dtype) for a in args[1:]]
        + [
            pltpu.VMEM((heads * rows, HD), f32),
            pltpu.VMEM((heads * rows, HD), f32),
            pltpu.VMEM((outer, half, width // outer), bf16),
            pltpu.SemaphoreType.DMA((10 + 3 * GROUPS,)),
        ],
        compiler_params=pltpu.CompilerParams(vmem_limit_bytes=56 * 1024 * 1024),
        cost_estimate=pl.CostEstimate(
            flops=2 * rows * heads * HD * (width + 2 * cache_len),
            bytes_accessed=bytes_read,
            transcendentals=rows * heads * cache_len,
        ),
        name="attention",
    )(*args)
    return payloads, new_key[:, None], new_value[:, None], new_logsum


def project_kernel(outer, inner, *refs):
    f32 = jnp.float32
    payload_refs, refs = refs[:outer], refs[outer:]
    weight_refs, refs = refs[:inner], refs[inner:]
    keep_ref, send_ref, hidden_ref, rows_buf, sums_buf = refs
    rows = rows_buf.shape[0] // outer
    half = payload_refs[0].shape[0] - rows
    part = hidden_ref.shape[1]
    depth = weight_refs[0].shape[0]
    is_first = lax.axis_index("tp") == 0
    index = lax.axis_index("ep")
    place, line = index // inner, index % inner
    for i, payload_ref in enumerate(payload_refs):
        at = place ^ i
        rows_buf[pl.ds(pl.multiple_of(at * rows, rows), rows), :] = payload_ref[:rows, :]
        hidden_ref[pl.ds(pl.multiple_of(at * half, half), half), :] = payload_ref[rows:, :part]
    for i, weight_ref in enumerate(weight_refs):
        sums_buf[line ^ i] = lax.dot_general(
            rows_buf[...], weight_ref[...], (((1,), (1,)), ((), ())), preferred_element_type=f32
        )
    for i in range(inner):
        lanes = slice(i * depth, (i + 1) * depth)
        for k in range(outer):
            low = sums_buf[i, k * rows : k * rows + half, :]
            high = sums_buf[i, k * rows + half : (k + 1) * rows, :]
            at = slice(k * half, (k + 1) * half)
            keep_ref[at, lanes] = jnp.where(is_first, low, high)
            send_ref[at, lanes] = jnp.where(is_first, high, low)


def project(payloads, weights, half):
    f32, bf16 = jnp.float32, jnp.bfloat16
    outer, inner = len(payloads), len(weights)
    rows = payloads[0].shape[0] - half
    depth, width = weights[0].shape
    vmem = pl.BlockSpec(memory_space=pltpu.VMEM)
    total = jax.ShapeDtypeStruct((outer * half, inner * depth), f32)
    return pl.pallas_call(
        functools.partial(project_kernel, outer, inner),
        out_shape=(total, total, jax.ShapeDtypeStruct(total.shape, bf16)),
        in_specs=[vmem] * (outer + inner),
        out_specs=(vmem,) * 3,
        scratch_shapes=[
            pltpu.VMEM((outer * rows, width), bf16),
            pltpu.VMEM((inner, outer * rows, depth), f32),
        ],
        compiler_params=pltpu.CompilerParams(vmem_limit_bytes=VMEM_LIMIT),
        cost_estimate=pl.CostEstimate(
            flops=2 * outer * rows * width * inner * depth,
            bytes_accessed=2 * (outer * rows + inner * depth) * width,
            transcendentals=0,
        ),
        name="project",
    )(*payloads, *weights)


def experts_kernel(outer, inner, blocks_ref, gain_ref, gate_ref, up_ref, down_ref, *refs):
    f32, bf16 = jnp.float32, jnp.bfloat16
    far_refs, (out_ref, own_ref, inputs_buf, sums_buf, *bufs, sems) = refs[:3], refs[3:]
    _, group, part = blocks_ref.shape
    half = group // outer
    width = outer * part
    fetches = [
        pltpu.make_async_copy(far, buf, sems.at[i])
        for i, (far, buf) in enumerate(zip(far_refs, bufs, strict=True))
    ]
    for fetch in fetches:
        fetch.start()
    gate_other, up_other, down_other = bufs
    index = lax.axis_index("ep")
    place, line = index // inner, index % inner
    gain = gain_ref[...].astype(f32).reshape(1, width)
    own_rows = pl.ds(pl.multiple_of(place * half, half), half)
    for z in range(outer):
        lanes = slice(z * part, (z + 1) * part)
        own_ref[:, lanes] = blocks_ref[z * inner + line, own_rows, :]
    for p in range(inner):
        squares = jnp.zeros((group, 1), f32)
        for z in range(outer):
            floats = blocks_ref[z * inner + p].astype(f32)
            squares = squares + jnp.sum(floats * floats, axis=-1, keepdims=True)
        inv_root = lax.rsqrt(squares / width + epsilon)
        for z in range(outer):
            lanes = slice(z * part, (z + 1) * part)
            floats = blocks_ref[z * inner + p].astype(f32)
            inputs_buf[p * group : (p + 1) * group, lanes] = (
                floats * inv_root * gain[:, lanes]
            ).astype(bf16)

    def act(gate_at, up_at):
        gate = jnp.dot(inputs_buf[...], gate_at[...], preferred_element_type=f32)
        up = jnp.dot(inputs_buf[...], up_at[...], preferred_element_type=f32)
        return (gate / (1.0 + jnp.exp(-gate)) * up).astype(bf16)

    for expert in range(gate_ref.shape[0]):
        near_act = act(gate_ref.at[expert], up_ref.at[expert])
        sums_buf[...] = jnp.dot(near_act, down_ref[expert], preferred_element_type=f32)
        if expert == 0:
            fetches[0].wait()
            fetches[1].wait()
        far_act = act(gate_other.at[expert], up_other.at[expert])
        if expert == 0:
            fetches[2].wait()
        total = sums_buf[...] + jnp.dot(
            far_act, down_other[expert], preferred_element_type=f32
        )
        for p in range(inner):
            for z in range(outer):
                at = p * group + z * half
                out_ref[z * inner + p, expert] = total[at : at + half].astype(bf16)


def experts(blocks, gain, own, other, outer, inner):
    bf16 = jnp.bfloat16
    ep_size, group, part = blocks.shape
    width = outer * part
    half = group // outer
    rows = ep_size * half
    local, _, depth = own[0].shape
    vmem = pl.BlockSpec(memory_space=pltpu.VMEM)
    outside = pl.BlockSpec(memory_space=pl.ANY)
    return pl.pallas_call(
        functools.partial(experts_kernel, outer, inner),
        out_shape=(
            jax.ShapeDtypeStruct((ep_size, local, half, width), bf16),
            jax.ShapeDtypeStruct((half, width), bf16),
        ),
        in_specs=[vmem] * 5 + [outside] * 3,
        out_specs=(vmem,) * 2,
        scratch_shapes=[
            pltpu.VMEM((rows, width), bf16),
            pltpu.VMEM((rows, width), jnp.float32),
            *(pltpu.VMEM(w.shape, bf16) for w in other),
            pltpu.SemaphoreType.DMA((3,)),
        ],
        compiler_params=pltpu.CompilerParams(vmem_limit_bytes=EXPERTS_LIMIT),
        cost_estimate=pl.CostEstimate(
            flops=12 * local * rows * width * depth,
            bytes_accessed=2 * (2 * rows * width + 6 * local * width * depth),
            transcendentals=2 * local * rows * depth,
        ),
        name="experts",
    )(blocks, gain, *own, *other)


def combine_kernel(returned_ref, ids_ref, scores_ref, own_ref, out_ref):
    f32 = jnp.float32
    ep_size, local, half, width = returned_ref.shape
    top, rows = ids_ref.shape
    square = (rows, rows)
    same = lax.broadcasted_iota(jnp.int32, square, 0) == lax.broadcasted_iota(jnp.int32, square, 1)
    turn = functools.partial(
        lax.dot_general,
        same.astype(f32),
        dimension_numbers=(((1,), (1,)), ((), ())),
        preferred_element_type=f32,
        precision=lax.Precision.HIGHEST,
    )
    scores = scores_ref[...]
    ids = turn(ids_ref[...].astype(f32))
    route = turn(scores / jnp.sum(scores, axis=0, keepdims=True))
    is_first = lax.axis_index("tp") == 0
    ids = jnp.where(is_first, ids[:half], ids[half:])
    route = jnp.where(is_first, route[:half], route[half:])
    expert = lax.broadcasted_iota(jnp.int32, (half, ep_size * local), 1).astype(f32)
    weight = jnp.zeros((half, ep_size * local), f32)
    for k in range(top):
        weight = weight + jnp.where(ids[:, k : k + 1] == expert, route[:, k : k + 1], 0.0)
    total = own_ref[...].astype(f32)
    mix = jnp.zeros((half, width), f32)
    for e in range(ep_size):
        for i in range(local):
            at = e * local + i
            mix = mix + returned_ref[e, i].astype(f32) * weight[:, at : at + 1]
    out_ref[...] = (total + mix).astype(out_ref.dtype)


def combine(returned, ids, scores, own):
    vmem = pl.BlockSpec(memory_space=pltpu.VMEM)
    return pl.pallas_call(
        combine_kernel,
        out_shape=jax.ShapeDtypeStruct(own.shape, own.dtype),
        in_specs=[vmem] * 4,
        out_specs=vmem,
        compiler_params=pltpu.CompilerParams(vmem_limit_bytes=VMEM_LIMIT),
        cost_estimate=pl.CostEstimate(
            flops=2 * returned.size, bytes_accessed=2 * returned.size, transcendentals=0
        ),
        name="combine",
    )(returned, ids.T, scores.T, own)


def over_lines(arrays, inner):
    ep_size, outer = lax.axis_size("ep"), len(arrays)
    if outer <= 4:
        return arrays[:1] + [
            lax.ppermute(a, "ep", [(e, e ^ (i * inner)) for e in range(ep_size)])
            for i, a in list(enumerate(arrays))[1:]
        ]
    place = lax.axis_index("ep") // inner
    order = jnp.arange(outer, dtype=jnp.int32) ^ place
    groups = [[z * inner + p for z in range(outer)] for p in range(inner)]
    moved = lax.all_to_all(
        jnp.stack(arrays)[order], "ep", 0, 0, axis_index_groups=groups, tiled=True
    )
    return list(moved[order])


def per_device(
    hidden,
    attn_gain,
    query_weight,
    key_weight,
    value_weight,
    forget_weight,
    forget_bias,
    cache_keys,
    cache_values,
    cache_logsum,
    lengths,
    out_weight,
    ffn_gain,
    expert_ids,
    expert_scores,
    gate_weights,
    up_weights,
    down_weights,
):
    f32, bf16 = jnp.float32, jnp.bfloat16
    rows_here, width = hidden.shape
    ep_size, tp_size = lax.axis_size("ep"), lax.axis_size("tp")
    tp_index = lax.axis_index("tp")
    is_first = tp_index == 0
    half = rows_here // tp_size
    local_experts = gate_weights.shape[0]

    gate_other = lax.ppermute(gate_weights, "tp", SWAP)
    up_other = lax.ppermute(up_weights, "tp", SWAP)
    down_other = lax.ppermute(down_weights, "tp", SWAP)

    inner = 4 if ep_size % 4 == 0 else 1
    outer = ep_size // inner
    heads_here = query_weight.shape[1]
    with jax.named_scope("share"):
        weight_half = lax.dynamic_slice_in_dim(out_weight, tp_index * heads_here, heads_here, 1)
        shared = [weight_half] + [
            lax.ppermute(weight_half, "ep", [(e, e ^ i) for e in range(ep_size)])
            for i in range(1, inner)
        ]
    with jax.named_scope("attend"):
        payloads, key_new, value_new, new_logsum = attention(
            hidden,
            attn_gain,
            query_weight,
            key_weight,
            value_weight,
            forget_weight,
            forget_bias,
            cache_keys,
            cache_values,
            cache_logsum,
            lengths,
            outer,
        )
    payloads[0] = payloads[0].astype(bf16)
    with jax.named_scope("lines"):
        payloads = over_lines(payloads, inner)
    keep, send, hidden_part = project(payloads, shared, half)
    mixed = (keep + lax.ppermute(send, "tp", SWAP)).astype(bf16)
    residual_part = (hidden_part.astype(f32) + mixed.astype(f32)).astype(bf16)

    residual_part, gate_other, up_other, down_other = lax.optimization_barrier(
        (residual_part, gate_other, up_other, down_other)
    )
    blocks = lax.all_to_all(
        jnp.broadcast_to(residual_part[None], (ep_size,) + residual_part.shape),
        "ep",
        split_axis=0,
        concat_axis=0,
        tiled=True,
    )
    outgoing, own = experts(
        blocks,
        ffn_gain,
        (gate_weights, up_weights, down_weights),
        (gate_other, up_other, down_other),
        outer,
        inner,
    )
    returned = lax.all_to_all(outgoing, "ep", split_axis=0, concat_axis=0, tiled=True)

    updated_mine = combine(returned, expert_ids, expert_scores, own)
    updated_theirs = lax.ppermute(updated_mine, "tp", SWAP)
    updated = jnp.concatenate(
        [
            jnp.where(is_first, updated_mine, updated_theirs),
            jnp.where(is_first, updated_theirs, updated_mine),
        ],
        axis=0,
    )
    return (updated, key_new, value_new, new_logsum)
def solution(mesh):
    in_specs = (
        P("ep", None),
        P(),
        P(None, "tp"),
        P(None, "tp"),
        P(None, "tp"),
        P(None, "tp"),
        P("tp"),
        P("ep", "tp", None, None),
        P("ep", "tp", None, None),
        P("ep", "tp", None),
        P("ep"),
        P("ep", None),
        P(),
        P("ep", None),
        P("ep", None),
        P("ep", None, "tp"),
        P("ep", None, "tp"),
        P("ep", "tp", None),
    )
    out_specs = (P("ep", None), P("ep", "tp", None), P("ep", "tp", None), P("ep", "tp"))
    return jax.shard_map(
        per_device, mesh=mesh, in_specs=in_specs, out_specs=out_specs, check_vma=False
    )
```
